512 devices in a mesh: sp: 64 (over z, y), tp: 8 (over x, core).
Axes of the slice: x: 4, y: 8, z: 8, core: 2. Of those that a mesh axis runs over, the one named last changes fastest.
Arguments:
- tokens: bfloat16 [16384, 2048], P('sp', 'tp'), may hold values from -6 to 6
- norm_gain: float32 [2048], replicated, may hold values from 0.1 to 1.9
- recur_query: bfloat16 [2048, 1024], P(None, 'tp'), may hold values from -0.125 to 0.125
- recur_forget: bfloat16 [2048, 1024], P(None, 'tp'), may hold values from -0.125 to 0.125
- recur_value: bfloat16 [2048, 1024], P(None, 'tp'), may hold values from -0.125 to 0.125
- gate_floor: float32 [1024], P('tp'), may hold values from 0.5 to 1
- extra_decay: float32 [16384, 8], P('sp', 'tp'), may hold values from 0 to 2
- start_state: float32 [8, 128, 128], P('tp'), may hold values from -0.0625 to 0.0625
- recur_gain: float32 [1024], P('tp'), may hold values from 0.1 to 1.9
- attend_query: bfloat16 [2048, 1024], P(None, 'tp')
- attend_key: bfloat16 [2048, 1024], P(None, 'tp')
- attend_value: bfloat16 [2048, 1024], P(None, 'tp'), may hold values from -0.125 to 0.125
- gate_cache: float32 [16384, 16], P(None, 'tp'), may hold values from -16384 to 0, as said below
- attend_gain: float32 [1024], P('tp'), may hold values from 0.1 to 1.9
- recur_output: bfloat16 [1024, 2048], P(None, 'tp'), may hold values from -0.1875 to 0.1875
- attend_output: bfloat16 [1024, 2048], P(None, 'tp'), may hold values from -0.1875 to 0.1875
Outputs:
- layer_output: bfloat16 [16384, 2048], P('sp', 'tp')
The draws below stay inside these ranges and needn't reach their ends.
Inputs may be any that keep to these rules, and one draw needn't show every extreme that they name: `gate_cache`: never rising along positions.
All inputs are finite; a program needn't handle non-finite values.
Results may differ from the reference program's by a relative error of at most 0.018.
Values may be sent and summed in bfloat16 or wider, within the bound.
A program may use at most 64 MiB of HBM per device.

```python
import jax
import jax.numpy as jnp
from jax import lax

D = 2048
RECUR_HEAD_COUNT = 8
KD = 128
VD = 128
FORGET_HEAD_COUNT = 16
FD = 64
TOK_DEV = 256
TOKEN_COUNT = 16384


def fast_heads(key, total_amount):
    order = jax.random.permutation(key, total_amount)
    return order < total_amount // 2


def spike_rates(key, total_amount):
    blocks = TOKEN_COUNT // TOK_DEV
    factor = jnp.exp(jax.random.uniform(jax.random.fold_in(key, 1), (blocks, 1, total_amount), jnp.float32, 0.0, jnp.log(4.0)))
    jitter = jax.random.uniform(jax.random.fold_in(key, 2), (blocks, TOK_DEV, total_amount), jnp.float32, 0.5, 1.5)
    steady_value = 0.3 / TOKEN_COUNT * factor * jitter
    spot_index = jax.random.randint(jax.random.fold_in(key, 3), (2, total_amount), 0, TOKEN_COUNT)
    block_sizes = jax.random.uniform(jax.random.fold_in(key, 4), (2, total_amount), jnp.float32, 0.22, 0.69)
    place_index = jnp.arange(TOKEN_COUNT)[:, None, None]
    spike_list = jnp.sum(jnp.where(place_index == spot_index[None], block_sizes[None], 0.0), axis=1)
    return steady_value.reshape(TOKEN_COUNT, total_amount) + spike_list


def draw_gate_floor(key, part):
    quick = fast_heads(jax.random.fold_in(key, 1), RECUR_HEAD_COUNT)
    slow_gap = jnp.exp(jax.random.uniform(jax.random.fold_in(key, 2), (RECUR_HEAD_COUNT, KD), jnp.float32, jnp.log(0.2), jnp.log(0.8))) / TOKEN_COUNT
    quick_floor = jax.random.uniform(jax.random.fold_in(key, 3), (RECUR_HEAD_COUNT, KD), jnp.float32, 0.8, 0.95)
    floors = jnp.where(quick[:, None], quick_floor, 1.0 - slow_gap)
    return floors.reshape(RECUR_HEAD_COUNT * KD)


def draw_extra_decay(key, part):
    return spike_rates(jax.random.fold_in(key, 5), RECUR_HEAD_COUNT)


def draw_gate_cache(key, part):
    gradual_steps = spike_rates(jax.random.fold_in(key, 6), FORGET_HEAD_COUNT)
    quick = fast_heads(jax.random.fold_in(key, 7), FORGET_HEAD_COUNT)
    blocks = TOKEN_COUNT // TOK_DEV
    factor = jnp.exp(jax.random.uniform(jax.random.fold_in(key, 8), (blocks, 1, FORGET_HEAD_COUNT), jnp.float32, 0.0, jnp.log(4.0)))
    rates = jax.random.uniform(jax.random.fold_in(key, 9), (blocks, TOK_DEV, FORGET_HEAD_COUNT), jnp.float32, 0.005, 0.02)
    quick_steps = (rates * factor).reshape(TOKEN_COUNT, FORGET_HEAD_COUNT)
    steps_all = jnp.where(quick[None, :], quick_steps, gradual_steps)
    return -jnp.cumsum(steps_all, axis=0)


def key_base(key):
    return jax.random.normal(jax.random.fold_in(key, 21), (D, FORGET_HEAD_COUNT * FD), jnp.float32) / jnp.sqrt(1.0 * D)


def draw_attend_key(key, part):
    return key_base(key).astype(jnp.bfloat16)


def draw_attend_query(key, part):
    fresh = jax.random.normal(jax.random.fold_in(key, 22), (D, FORGET_HEAD_COUNT * FD), jnp.float32) / jnp.sqrt(1.0 * D)
    return fresh.astype(jnp.bfloat16)


def level_of(rng, shape, split, least, high):
    factor_of = 1.0
    for position, blocks in split:
        steps = jax.random.uniform(jax.random.fold_in(jax.random.fold_in(rng, 6), position), (blocks,), jnp.float32, least / len(split), high / len(split))
        factor_of = factor_of * jnp.repeat(jnp.exp(steps), shape[position] // blocks).reshape((-1,) + (1,) * (len(shape) - 1 - position))
    return factor_of


def centred(key, extent, deviation, limit, split=(), held_as=jnp.bfloat16):
    result = jax.random.normal(key, extent, jnp.float32) * deviation
    if len(split) > 0:
        result = level_of(key, extent, split, -0.22, 0.18) * result
    return jnp.clip(result, min=-limit, max=limit).astype(held_as)


def setup_inputs(seed: int = 0) -> dict:
    keys = jax.random.split(jax.random.key(seed), 17)
    tokens = centred(keys[0], (TOKEN_COUNT, D), 1.0, 6.0, ((0, 64), (1, 8)))
    norm_gain = jnp.clip(1.0 + 0.18 * jax.random.normal(keys[1], (D,), jnp.float32), 0.1, 1.9)
    recur_query = centred(keys[2], (D, RECUR_HEAD_COUNT * KD), D ** -0.5, 0.125, ((1, 8),))
    recur_forget = centred(keys[3], (D, RECUR_HEAD_COUNT * KD), D ** -0.5, 0.125, ((1, 8),))
    recur_value = centred(keys[4], (D, RECUR_HEAD_COUNT * VD), D ** -0.5, 0.125, ((1, 8),))
    gate_floor = draw_gate_floor(jax.random.fold_in(keys[16], 71), 0)
    extra_decay = draw_extra_decay(jax.random.fold_in(keys[16], 71), 0)
    start_state = centred(keys[7], (RECUR_HEAD_COUNT, KD, VD), (0.5 / TOKEN_COUNT ** 0.5), 0.0625, ((0, 8),), jnp.float32)
    recur_gain = jnp.clip(1.0 + 0.18 * jax.random.normal(keys[8], (RECUR_HEAD_COUNT * VD,), jnp.float32), 0.1, 1.9)
    attend_query = draw_attend_query(jax.random.fold_in(keys[16], 71), 0)
    attend_key = draw_attend_key(jax.random.fold_in(keys[16], 71), 0)
    attend_value = centred(keys[11], (D, FORGET_HEAD_COUNT * FD), D ** -0.5, 0.125, ((1, 8),))
    gate_cache = draw_gate_cache(jax.random.fold_in(keys[16], 71), 0)
    attend_gain = jnp.clip(1.0 + 0.18 * jax.random.normal(keys[13], (FORGET_HEAD_COUNT * FD,), jnp.float32), 0.1, 1.9)
    recur_output = centred(keys[14], (RECUR_HEAD_COUNT * VD, D), (RECUR_HEAD_COUNT * VD) ** -0.5, 0.1875, ((1, 8),))
    attend_output = centred(keys[15], (FORGET_HEAD_COUNT * FD, D), (FORGET_HEAD_COUNT * FD) ** -0.5, 0.1875, ((1, 8),))
    return {"tokens": tokens, "norm_gain": norm_gain, "recur_query": recur_query, "recur_forget": recur_forget, "recur_value": recur_value, "gate_floor": gate_floor, "extra_decay": extra_decay, "start_state": start_state, "recur_gain": recur_gain, "attend_query": attend_query, "attend_key": attend_key, "attend_value": attend_value, "gate_cache": gate_cache, "attend_gain": attend_gain, "recur_output": recur_output, "attend_output": attend_output}


EPSILON = 1e-06
TOP_PRECISION = lax.Precision.HIGHEST

def head_norm(per_head, head_gain):
    normed = per_head * lax.rsqrt(lax.optimization_barrier(jnp.mean(per_head * per_head, axis=-1, keepdims=True)) + EPSILON)
    return normed.reshape(per_head.shape[0], -1) * head_gain

def recurrence(query_rows, decays, inflow, values, initial):
    span_len = 64
    blocks = query_rows.shape[0] // span_len

    def to_blocks(tensor):
        return tensor.reshape(blocks, span_len, tensor.shape[1], tensor.shape[2])
    causal = jnp.tril(jnp.ones((span_len, span_len), dtype=bool))[:, :, None, None]

    def advance(carried_state, pieces):
        query_block, g_block, k_block, value_block = pieces
        running_total = jnp.cumsum(g_block, axis=0)
        offsets = jnp.where(causal, running_total[:, None] - running_total[None, :], -jnp.inf)
        mixing = jnp.einsum('thk,shk,tshk->hts', query_block, k_block, jnp.exp(offsets), precision=TOP_PRECISION)
        final_result = jnp.einsum('hts,shv->thv', mixing, value_block, precision=TOP_PRECISION)
        final_result = final_result + jnp.einsum('dzc,zcu->dzu', query_block * jnp.exp(running_total), carried_state, precision=TOP_PRECISION)
        ending_state = running_total[-1]
        weighted_values = k_block * jnp.exp(ending_state[None] - running_total)
        carried_state = jnp.exp(ending_state)[..., None] * carried_state + jnp.einsum('cun,cub->unb', weighted_values, value_block, precision=TOP_PRECISION)
        return (carried_state, final_result)
    _, results = lax.scan(advance, initial, (to_blocks(query_rows), to_blocks(decays), to_blocks(inflow), to_blocks(values)))
    return results.reshape(query_rows.shape[0], query_rows.shape[1], values.shape[2])

def attention(query_rows, key_rows, value_rows, gate_sums):
    length = query_rows.shape[0]
    height = min(256, length)
    blocks = length // height
    scaling = query_rows.shape[2] ** (-0.5)
    key_index = jnp.arange(length)
    keys_wide = key_rows.astype(jnp.float32)
    values_wide = value_rows.astype(jnp.float32)

    def one_block(number):
        first_row = number * height
        query_block = lax.dynamic_slice_in_dim(query_rows, first_row, height, 0).astype(jnp.float32)
        g_block = lax.dynamic_slice_in_dim(gate_sums, first_row, height, 0)
        scores = jnp.einsum('qhd,khd->hqk', query_block, keys_wide) * scaling
        scores = scores + g_block.T[:, :, None] - gate_sums.T[:, None, :]
        query_index = first_row + jnp.arange(height)
        allowed = key_index[None, :] <= query_index[:, None]
        scores = jnp.where(allowed[None], scores, -jnp.inf)
        maxima = lax.optimization_barrier(jnp.max(scores, axis=-1, keepdims=True))
        weights = jnp.exp(scores - maxima)
        totals = lax.optimization_barrier(jnp.sum(weights, axis=-1))
        rounded = lax.optimization_barrier(weights.astype(jnp.bfloat16)).astype(jnp.float32)
        summed = jnp.einsum('hqk,khd->qhd', rounded, values_wide)
        return summed / totals.T[:, :, None]
    results = lax.map(one_block, jnp.arange(blocks))
    return results.reshape(length, query_rows.shape[1], query_rows.shape[2])

def reference(tokens, norm_gain, recur_query, recur_forget, recur_value, gate_floor, extra_decay, start_state, recur_gain, attend_query, attend_key, attend_value, gate_cache, attend_gain, recur_output, attend_output):
    length = tokens.shape[0]
    wide = tokens.astype(jnp.float32)
    inverse = lax.rsqrt(lax.optimization_barrier(jnp.mean(wide * wide, axis=1, keepdims=True)) + EPSILON)
    scaled = (wide * norm_gain).astype(jnp.bfloat16)

    def project(weight):
        return (jnp.dot(scaled, weight, preferred_element_type=jnp.float32) * inverse).astype(jnp.bfloat16)
    rec_heads = start_state.shape[0]
    query_rows = project(recur_query).astype(jnp.float32).reshape(length, rec_heads, -1)
    forget_pre = project(recur_forget).astype(jnp.float32).reshape(length, rec_heads, -1)
    values = project(recur_value).astype(jnp.float32).reshape(length, rec_heads, -1)
    inflow = (1.0 - gate_floor.reshape(rec_heads, -1)) * jax.nn.sigmoid(-forget_pre)
    decays = jnp.log1p(-inflow) - extra_decay[:, :, None]
    rec_out = recurrence(query_rows, decays, inflow, values, start_state)
    rec_rows = head_norm(rec_out, recur_gain).astype(jnp.bfloat16)
    att_heads = gate_cache.shape[1]
    att_query = project(attend_query).reshape(length, att_heads, -1)
    att_key = project(attend_key).reshape(length, att_heads, -1)
    att_value = project(attend_value).reshape(length, att_heads, -1)
    att_out = attention(att_query, att_key, att_value, gate_cache)
    att_rows = head_norm(att_out, attend_gain).astype(jnp.bfloat16)
    combined = jnp.dot(rec_rows, recur_output, preferred_element_type=jnp.float32)
    combined = combined + jnp.dot(att_rows, attend_output, preferred_element_type=jnp.float32)
    return combined.astype(jnp.bfloat16)
```

```python
import functools

import jax
import jax.numpy as jnp
from jax import lax
from jax.experimental import pallas as pl
from jax.experimental.pallas import tpu as pltpu
from jax.sharding import Mesh
from jax.sharding import PartitionSpec as P

FD = 64
SP = ("z", "y")
TP = ("x", "c")
EPSILON = 1e-06
LOW = -1e30
SUB = 16
F32 = jnp.float32
BF16 = jnp.bfloat16
MESH = pl.DeviceIdType.MESH
VMEM_LIMIT = 60 * 1024 * 1024


def remote(src, dst, send, recv, device):
    return pltpu.make_async_remote_copy(
        src_ref=src, dst_ref=dst, send_sem=send, recv_sem=recv, device_id=device, device_id_type=MESH
    )


def tp_greet(nx):
    x, c = lax.axis_index("x"), lax.axis_index("c")
    barrier = pltpu.get_barrier_semaphore()
    peers = [{"c": 1 - c}, {"x": lax.rem(x + 1, nx)}, {"x": lax.rem(x + nx - 1, nx)}]
    for peer in peers:
        pl.semaphore_signal(barrier, inc=1, device_id=peer, device_id_type=MESH)
    pl.semaphore_wait(barrier, len(peers))


def tp_gather(nx, slots, send_sem, recv_sem, consume):
    x, c = lax.axis_index("x"), lax.axis_index("c")
    other = 1 - c
    right, left, far = lax.rem(x + 1, nx), lax.rem(x + nx - 1, nx), lax.rem(x + 2, nx)
    half = slots.shape[1] // 2
    me = 2 * x + c
    top, bottom = pl.ds(0, half), pl.ds(half, half)

    def piece(number, p, rows, device):
        ref = slots.at[p] if rows is None else slots.at[p, rows]
        return remote(ref, ref, send_sem.at[number], recv_sem.at[number], device)

    to_right, to_left, to_other = {"x": right}, {"x": left}, {"c": other}
    from_left, from_right, across = 2 * left + c, 2 * right + c, 2 * far + c
    sends = [
        piece(0, me, top, to_right),
        piece(1, me, bottom, to_left),
        piece(2, me, bottom, to_right),
        piece(3, me, top, to_left),
        piece(4, me, None, to_other),
    ]
    for copy in sends:
        copy.start()
    consume(me)

    def forward(number, p, rows, device):
        copy = piece(number, p, rows, device)
        copy.start()
        sends.append(copy)

    piece(0, from_left, top, to_right).wait_recv()
    forward(5, from_left, top, to_right)
    piece(1, from_right, bottom, to_left).wait_recv()
    forward(6, from_right, bottom, to_left)
    piece(4, 2 * x + other, None, to_other).wait_recv()
    consume(2 * x + other)
    piece(2, from_left, bottom, to_right).wait_recv()
    forward(7, from_left, None, to_other)
    piece(3, from_right, top, to_left).wait_recv()
    forward(8, from_right, None, to_other)
    consume(from_left)
    consume(from_right)
    piece(5, across, top, to_right).wait_recv()
    piece(6, across, bottom, to_left).wait_recv()
    forward(9, across, None, to_other)
    piece(7, 2 * left + other, None, to_other).wait_recv()
    consume(2 * left + other)
    piece(8, 2 * right + other, None, to_other).wait_recv()
    consume(2 * right + other)
    consume(across)
    piece(9, 2 * far + other, None, to_other).wait_recv()
    consume(2 * far + other)
    for copy in sends:
        copy.wait_send()


def project_kernel(
    nx, tokens_ref, gain_ref, *refs
):
    weights, out_ref = refs[:6], refs[6]
    slots, held, total, squares, local_sem, weight_sem, send_sem, recv_sem = refs[7:]
    x, c = lax.axis_index("x"), lax.axis_index("c")
    own = pltpu.make_async_copy(tokens_ref, slots.at[2 * x + c], local_sem)
    own.start()
    width = weights[0].shape[1]
    loads = [
        pltpu.make_async_copy(ref, held.at[:, pl.ds(n * width, width)], weight_sem.at[n])
        for n, ref in enumerate(weights)
    ]
    for load in loads:
        load.start()
    total[...] = jnp.zeros_like(total)
    squares[...] = jnp.zeros_like(squares)
    tp_greet(nx)
    own.wait()
    features = tokens_ref.shape[1]
    waited = []

    def consume(p):
        if not waited:
            for load in loads:
                load.wait()
            waited.append(True)
        wide = slots[p].astype(F32)
        squared = wide * wide
        folded = squared[:, :128]
        for k in range(1, features // 128):
            folded = folded + squared[:, k * 128 : (k + 1) * 128]
        squares[...] += folded
        scaled = (wide * gain_ref[p]).astype(BF16)
        rows = pl.ds(pl.multiple_of(p * features, features), features)
        total[...] += jnp.dot(scaled, held[rows, :], preferred_element_type=F32)

    tp_gather(nx, slots, send_sem, recv_sem, consume)
    mean = jnp.sum(squares[...], axis=1, keepdims=True) / held.shape[0]
    inverse = lax.rsqrt(mean + EPSILON)
    out_ref[...] = (total[...] * inverse).astype(BF16)


def output_kernel(nx, rows_ref, recur_ref, attend_ref, out_ref, slots, held, total, local_sem, weight_sem, send_sem, recv_sem):
    x, c = lax.axis_index("x"), lax.axis_index("c")
    own = pltpu.make_async_copy(rows_ref, slots.at[2 * x + c], local_sem)
    own.start()
    depth = rows_ref.shape[1] // 2
    pieces = 2 * nx
    loads = []
    for n in range(pieces):
        for k, ref in enumerate((recur_ref, attend_ref)):
            loads.append(
                pltpu.make_async_copy(
                    ref.at[pl.ds(n * depth, depth)], held.at[n, pl.ds(k * depth, depth)], weight_sem.at[2 * n + k]
                )
            )
    for load in loads:
        load.start()
    total[...] = jnp.zeros_like(total)
    tp_greet(nx)
    own.wait()
    waited = []

    def consume(p):
        if not waited:
            for load in loads:
                load.wait()
            waited.append(True)
        total[...] += jnp.dot(slots[p], held[p], preferred_element_type=F32)

    tp_gather(nx, slots, send_sem, recv_sem, consume)
    out_ref[...] = total[...].astype(BF16)


def thirds(value):
    first = value.astype(BF16)
    rest = value - first.astype(F32)
    second = rest.astype(BF16)
    third = (rest - second.astype(F32)).astype(BF16)
    return first, second, third


def whole(first, second, third):
    return first.astype(F32) + second.astype(F32) + third.astype(F32)


def padded_thirds(rows, height):
    parts = [part.astype(F32) for row in rows for part in thirds(row)]
    parts.append(jnp.zeros((height - len(parts), rows[0].shape[1]), F32))
    return jnp.concatenate(parts, axis=0).astype(BF16)


def nt(left, right):
    return lax.dot_general(left, right, (((1,), (1,)), ((), ())), preferred_element_type=F32)


def middle_kernel(
    nz,
    ny,
    proj_ref,
    floor_ref,
    decay_ref,
    start_ref,
    recur_gain_ref,
    gate_ref,
    attend_gain_ref,
    out_ref,
    kbuf,
    vbuf,
    qbuf,
    sbuf,
    tbuf,
    obuf,
    rbuf,
    acc,
    top,
    bias,
    kv_send,
    kv_recv,
    q_send,
    q_recv,
    t_send,
    t_recv,
    o_send,
    o_recv,
):
    z, y = lax.axis_index("z"), lax.axis_index("y")
    height = proj_ref.shape[0]
    row_at = z * ny * height

    def gates(zq, yq):
        at = pl.multiple_of((zq * ny + yq) * height, height)
        return gate_ref[:, pl.ds(at, height)]

    barrier = pltpu.get_barrier_semaphore()
    for step in (1, ny - 1):
        pl.semaphore_signal(barrier, inc=1, device_id={"y": lax.rem(y + step, ny)}, device_id_type=MESH)
    for step in range(1, nz):
        pl.semaphore_signal(barrier, inc=1, device_id={"z": lax.rem(z + step, nz)}, device_id_type=MESH)

    kbuf[y] = proj_ref[:, 512:640]
    values_t = jnp.transpose(proj_ref[:, 640:768].astype(F32))
    vbuf[y] = values_t.astype(BF16)
    query_t = jnp.transpose(proj_ref[:, 384:512].astype(F32) * (FD**-0.5))
    qbuf[z] = query_t.astype(BF16)
    pl.semaphore_wait(barrier, nz + 1)

    y_next, y_last = {"y": lax.rem(y + 1, ny)}, {"y": lax.rem(y + ny - 1, ny)}
    z_next, z_last = {"z": lax.rem(z + 1, nz)}, {"z": lax.rem(z + nz - 1, nz)}
    kv = (kbuf, vbuf, sbuf)

    def y_copy(way, unit, slot, step):
        device = y_next if way == 0 else y_last
        ref = kv[unit].at[slot]
        return remote(ref, ref, kv_send.at[way, unit, step], kv_recv.at[way, unit, step], device)

    def z_copy(way, slot, step):
        device = z_next if way == 0 else z_last
        ref = qbuf.at[slot]
        return remote(ref, ref, q_send.at[way, step], q_recv.at[way, step], device)

    def y_units(way, step):
        if 2 * step < ny:
            return (0, 1, 2)
        return (0, 2) if way == 0 else (1,)

    def y_slot(way, step):
        return lax.rem(y + ny - step, ny) if way == 0 else lax.rem(y + step, ny)

    def z_slot(way, step):
        return lax.rem(z + nz - step, nz) if way == 0 else lax.rem(z + step, nz)

    started = []

    def begin(copy):
        copy.start()
        started.append(copy)

    def y_begin(step, units):
        for unit in units:
            for way in (0, 1):
                if unit in y_units(way, step):
                    begin(y_copy(way, unit, y_slot(way, step - 1), step - 1))

    def z_ways(step):
        return (0, 1) if 2 * step < nz else (0,)

    y_begin(1, (0, 1))
    for way in z_ways(1):
        begin(z_copy(way, z, 0))

    queries = proj_ref[:, 0:128].astype(F32)
    forget = proj_ref[:, 128:256].astype(F32)
    values = proj_ref[:, 256:384]
    inflow = (1.0 - floor_ref[...]) / (1.0 + jnp.exp(forget))
    extra = jnp.transpose(jnp.broadcast_to(decay_ref[...], (128, height)))
    decays = jnp.log1p(-inflow) - extra
    rows_i = lax.broadcasted_iota(jnp.int32, (height, height), 0)
    cols_i = lax.broadcasted_iota(jnp.int32, (height, height), 1)
    lower = jnp.where(cols_i <= rows_i, 1.0, 0.0).astype(BF16)
    sums = jnp.zeros((height, 128), F32)
    for part in thirds(decays):
        sums = sums + jnp.dot(lower, part, preferred_element_type=F32)
    ending = sums[height - 1 : height, :]
    kept = (inflow * jnp.exp(ending - sums)).astype(BF16)
    values_rt = jnp.transpose(values.astype(F32)).astype(BF16)
    sbuf[y] = jnp.concatenate(
        [jnp.dot(values_rt, kept, preferred_element_type=F32).astype(BF16), padded_thirds([ending], 16)], axis=0
    )
    y_begin(1, (2,))
    mixing = []
    for at in range(0, height, SUB):
        reach = 128 if at + SUB <= 128 else height
        base = sums[at - 1 : at, :] if at else jnp.zeros((1, 128), F32)
        near = queries[at : at + SUB] * jnp.exp(sums[at : at + SUB] - base)
        past = inflow[:reach] * jnp.exp(jnp.minimum(base - sums[:reach], 60.0))
        piece = nt(near.astype(BF16), past.astype(BF16))
        if reach < height:
            piece = jnp.concatenate([piece, jnp.zeros((SUB, height - reach), F32)], axis=1)
        mixing.append(piece)
    mixing = jnp.where(cols_i <= rows_i, jnp.concatenate(mixing, axis=0), 0.0)
    local_out = jnp.dot(mixing.astype(BF16), values, preferred_element_type=F32)
    carried_query = (queries * jnp.exp(sums)).astype(BF16)

    reference_gate = gates(z, ny - 1)[:, height - 1 : height]
    for slot in range(ny):
        relative = reference_gate - gates(z, slot)
        for head in range(2):
            bias[slot, head] = jnp.transpose(jnp.broadcast_to(relative[head : head + 1], (128, height)))
    top[...] = jnp.full(top.shape, LOW, F32)
    acc[...] = jnp.zeros_like(acc)
    ones = jnp.ones((16, height), BF16)
    blank = jnp.zeros((FD, height), BF16)

    def update(zq, yk, own):
        keys = kbuf[yk]
        for head in range(2):
            part = qbuf[zq, head * FD : (head + 1) * FD]
            split = jnp.concatenate([part, blank] if head == 0 else [blank, part], axis=0)
            scores = jnp.dot(keys, split, preferred_element_type=F32)
            shift = bias[yk, head]
            scores = scores + jnp.concatenate([shift] * (height // 128), axis=1)
            if own:
                scores = jnp.where(rows_i <= cols_i, scores, LOW)
            old = top[zq, head]
            new = jnp.maximum(old, jnp.max(scores, axis=0, keepdims=True))
            weights = jnp.exp(scores - new[0:1])
            rescale = jnp.exp(old - new)[0:1]
            top[zq, head] = new
            left = jnp.concatenate([vbuf[yk, head * FD : (head + 1) * FD], ones], axis=0)
            acc[zq, head] = acc[zq, head] * rescale + jnp.dot(
                left, weights.astype(BF16), preferred_element_type=F32
            )

    update(z, y, True)

    def visit(oq, ok):
        zq, yk = lax.rem(z + oq + nz, nz), lax.rem(y + ok + ny, ny)
        needed = (zq > z) | ((zq == z) & (yk < y))

        @pl.when(needed)
        def _():
            update(zq, yk, False)

    for step in range(1, ny // 2 + 1):
        for unit in (0, 1, 2):
            for way in (0, 1):
                if unit in y_units(way, step):
                    slot = y_slot(way, step)
                    y_copy(way, unit, slot, step - 1).wait_recv()
                    if unit in y_units(way, step + 1) and step < ny // 2:
                        begin(y_copy(way, unit, slot, step))
        for way in z_ways(step):
            slot = z_slot(way, step)
            z_copy(way, slot, step - 1).wait_recv()
            if step < nz // 2 and way in z_ways(step + 1):
                begin(z_copy(way, slot, step))
        if step < ny // 2:

            def ring(n, carry, step=step):
                side, r = n // (2 * step), n % (2 * step)
                oq = jnp.where(side == 0, r - step, jnp.where(side == 1, step, jnp.where(side == 2, step - r, -step)))
                ok = jnp.where(side == 0, -step, jnp.where(side == 1, r - step, jnp.where(side == 2, step, step - r)))
                visit(oq, ok)
                return carry

            lax.fori_loop(0, 8 * step, ring, 0)
        else:
            state = jnp.zeros((128, 128), F32)
            inside = state
            log_all = jnp.zeros((1, 128), F32)
            log_before = log_all
            for slot in range(ny):
                block = sbuf[slot].astype(F32)
                log_own = block[128:129] + block[129:130] + block[130:131]
                state = state * jnp.exp(log_own) + block[:128]
                log_all = log_all + log_own
                inside = jnp.where(slot < y, state, inside)
                log_before = jnp.where(slot < y, log_all, log_before)
            tbuf[z] = jnp.concatenate([state.astype(BF16), padded_thirds([log_all], 16)], axis=0)

            def t_copy(slot, target):
                ref = tbuf.at[slot]
                return remote(ref, ref, t_send.at[target], t_recv.at[slot], {"z": target})

            @pl.loop(z + 1, nz)
            def _(target):
                t_copy(z, target).start()

            def last(n, carry, step=step):
                oq = jnp.where(n < 2 * step, n - step + 1, step)
                ok = jnp.where(n < 2 * step, step, n - 3 * step + 1)
                visit(oq, ok)
                return carry

            lax.fori_loop(0, 4 * step - 1, last, 0)

    def o_copy(source, slot, target):
        return remote(obuf.at[slot], rbuf.at[source], o_send.at[slot], o_recv.at[source], {"z": target})

    def logs_of(zq):
        shift = gates(zq, y) - reference_gate
        return [
            top[zq, head][0:1] + jnp.log(acc[zq, head][FD : FD + 1]) + shift[head : head + 1] for head in range(2)
        ]

    def rows_of(zq):
        return [acc[zq, head][:FD] / acc[zq, head][FD : FD + 1] for head in range(2)]

    @pl.loop(z + 1, nz)
    def _(target):
        obuf[target] = jnp.concatenate(
            [part.astype(BF16) for part in rows_of(target)] + [padded_thirds(logs_of(target), 16)], axis=0
        )
        o_copy(z, target, target).start()

    def take(slot, state):
        t_copy(slot, z).wait_recv()
        block = tbuf[slot].astype(F32)
        log_own = block[128:129] + block[129:130] + block[130:131]
        return state * jnp.exp(log_own) + block[:128]

    arriving = lax.fori_loop(0, z, take, jnp.transpose(start_ref[...]))
    arriving = arriving * jnp.exp(log_before) + inside
    rec_out = local_out + nt(carried_query, arriving.astype(BF16))
    mean = jnp.mean(rec_out * rec_out, axis=1, keepdims=True)
    out_ref[:, 0:128] = (rec_out * lax.rsqrt(mean + EPSILON) * recur_gain_ref[...]).astype(BF16)

    def merge(slot, carry):
        o_copy(slot, slot, z).wait_recv()
        block = rbuf[slot].astype(F32)
        merged = []
        for head in range(2):
            best, amount, rows = carry[3 * head : 3 * head + 3]
            at = 2 * FD + 3 * head
            log = block[at : at + 1] + block[at + 1 : at + 2] + block[at + 2 : at + 3]
            new = jnp.maximum(best, log)
            keep, add = jnp.exp(best - new), jnp.exp(log - new)
            merged += [new, amount * keep + add, rows * keep + block[head * FD : (head + 1) * FD] * add]
        return tuple(merged)

    own_logs, own_rows = logs_of(z), rows_of(z)
    start = []
    for head in range(2):
        start += [own_logs[head], jnp.ones((1, height), F32), own_rows[head]]
    merged = lax.fori_loop(0, z, merge, tuple(start))
    normed = []
    for head in range(2):
        rows = merged[3 * head + 2] / merged[3 * head + 1]
        mean = jnp.mean(rows * rows, axis=0, keepdims=True)
        normed.append(rows * lax.rsqrt(mean + EPSILON))
    att_rows = jnp.transpose(jnp.concatenate(normed, axis=0))
    out_ref[:, 128:256] = (att_rows * attend_gain_ref[...]).astype(BF16)

    for copy in started:
        copy.wait_send()

    @pl.loop(z + 1, nz)
    def _(target):
        t_copy(z, target).wait_send()
        o_copy(z, target, target).wait_send()


VM = pl.BlockSpec(memory_space=pltpu.VMEM)
ANY = pl.BlockSpec(memory_space=pl.ANY)
DMA = pltpu.SemaphoreType.DMA


def params(number):
    return pltpu.CompilerParams(collective_id=number, has_side_effects=True, vmem_limit_bytes=VMEM_LIMIT)


def project(nx, tokens, norm_gain, weights):
    height, features = tokens.shape
    model = norm_gain.shape[0]
    width = sum(weight.shape[1] for weight in weights)
    return pl.pallas_call(
        functools.partial(project_kernel, nx),
        out_shape=jax.ShapeDtypeStruct((height, width), BF16),
        in_specs=[ANY, VM] + [ANY] * 6,
        out_specs=VM,
        scratch_shapes=[
            pltpu.VMEM((2 * nx, height, features), BF16),
            pltpu.VMEM((model, width), BF16),
            pltpu.VMEM((height, width), F32),
            pltpu.VMEM((height, 128), F32),
            DMA,
            DMA((6,)),
            DMA((10,)),
            DMA((10,)),
        ],
        compiler_params=params(0),
        name="project",
    )(tokens, norm_gain.reshape(2 * nx, 1, features), *weights)


def middle(nz, ny, projected, gate_floor, extra_decay, start_state, recur_gain, gate_cache, attend_gain):
    height = projected.shape[0]
    return pl.pallas_call(
        functools.partial(middle_kernel, nz, ny),
        out_shape=jax.ShapeDtypeStruct((height, 256), BF16),
        in_specs=[VM] * 7,
        out_specs=VM,
        scratch_shapes=[
            pltpu.VMEM((ny, height, 128), BF16),
            pltpu.VMEM((ny, 128, height), BF16),
            pltpu.VMEM((nz, 128, height), BF16),
            pltpu.VMEM((ny, 144, 128), BF16),
            pltpu.VMEM((nz, 144, 128), BF16),
            pltpu.VMEM((nz, 144, height), BF16),
            pltpu.VMEM((nz, 144, height), BF16),
            pltpu.VMEM((nz, 2, FD + 16, height), F32),
            pltpu.VMEM((nz, 2, 8, height), F32),
            pltpu.VMEM((ny, 2, height, 128), F32),
            DMA((2, 3, ny // 2)),
            DMA((2, 3, ny // 2)),
            DMA((2, nz // 2)),
            DMA((2, nz // 2)),
            DMA((nz,)),
            DMA((nz,)),
            DMA((nz,)),
            DMA((nz,)),
        ],
        compiler_params=params(1),
        name="middle",
    )(
        projected,
        gate_floor.reshape(1, -1),
        extra_decay.reshape(1, -1),
        start_state.reshape(128, 128),
        recur_gain.reshape(1, -1),
        gate_cache.T,
        attend_gain.reshape(1, -1),
    )


def output(nx, rows, recur_output, attend_output):
    height = rows.shape[0]
    width = recur_output.shape[1]
    return pl.pallas_call(
        functools.partial(output_kernel, nx),
        out_shape=jax.ShapeDtypeStruct((height, width), BF16),
        in_specs=[ANY] * 3,
        out_specs=VM,
        scratch_shapes=[
            pltpu.VMEM((2 * nx, height, 256), BF16),
            pltpu.VMEM((2 * nx, 256, width), BF16),
            pltpu.VMEM((height, width), F32),
            DMA,
            DMA((4 * nx,)),
            DMA((10,)),
            DMA((10,)),
        ],
        compiler_params=params(2),
        name="output",
    )(rows, recur_output, attend_output)


def shards(
    sizes,
    tokens,
    norm_gain,
    recur_query,
    recur_forget,
    recur_value,
    gate_floor,
    extra_decay,
    start_state,
    recur_gain,
    attend_query,
    attend_key,
    attend_value,
    gate_cache,
    attend_gain,
    recur_output,
    attend_output,
):
    nz, ny, nx = sizes
    weights = (recur_query, recur_forget, recur_value, attend_query, attend_key, attend_value)
    projected = project(nx, tokens, norm_gain, weights)
    rows = middle(nz, ny, projected, gate_floor, extra_decay, start_state, recur_gain, gate_cache, attend_gain)
    return output(nx, rows, recur_output, attend_output)


def solution(mesh):
    sizes = (8, 8, 4)
    finer = Mesh(mesh.devices.reshape(*sizes, 2), ("z", "y", "x", "c"))
    return jax.shard_map(
        functools.partial(shards, sizes),
        mesh=finer,
        in_specs=(
            P(SP, TP),
            P(),
            P(None, TP),
            P(None, TP),
            P(None, TP),
            P(TP),
            P(SP, TP),
            P(TP, None, None),
            P(TP),
            P(None, TP),
            P(None, TP),
            P(None, TP),
            P(None, TP),
            P(TP),
            P(None, TP),
            P(None, TP),
        ),
        out_specs=P(SP, TP),
        check_vma=False,
    )
```

```python
import functools

import jax
import jax.numpy as jnp
from jax import lax
from jax.experimental import pallas as pl
from jax.experimental.pallas import tpu as pltpu
from jax.sharding import Mesh
from jax.sharding import PartitionSpec as P

FD = 64
SP = ("z", "y")
TP = ("x", "c")
EPSILON = 1e-06
LOW = -1e30
SUB = 16
LANES = 2
F32 = jnp.float32
BF16 = jnp.bfloat16
MESH = pl.DeviceIdType.MESH
VMEM_LIMIT = 60 * 1024 * 1024


def remote(src, dst, send, recv, device):
    return pltpu.make_async_remote_copy(
        src_ref=src, dst_ref=dst, send_sem=send, recv_sem=recv, device_id=device, device_id_type=MESH
    )


def tp_greet(nx):
    x, c = lax.axis_index("x"), lax.axis_index("c")
    barrier = pltpu.get_barrier_semaphore()
    peers = [{"c": 1 - c}, {"x": lax.rem(x + 1, nx)}, {"x": lax.rem(x + nx - 1, nx)}]
    for peer in peers:
        pl.semaphore_signal(barrier, inc=1, device_id=peer, device_id_type=MESH)
    pl.semaphore_wait(barrier, len(peers))


def tp_gather(nx, slots, send_sem, recv_sem, consume):
    x, c = lax.axis_index("x"), lax.axis_index("c")
    other = 1 - c
    right, left, far = lax.rem(x + 1, nx), lax.rem(x + nx - 1, nx), lax.rem(x + 2, nx)
    half = slots.shape[1] // 2
    me = 2 * x + c
    top, bottom = pl.ds(0, half), pl.ds(half, half)

    def piece(number, p, rows, device):
        ref = slots.at[p] if rows is None else slots.at[p, rows]
        return remote(ref, ref, send_sem.at[number], recv_sem.at[number], device)

    to_right, to_left, to_other = {"x": right}, {"x": left}, {"c": other}
    from_left, from_right, across = 2 * left + c, 2 * right + c, 2 * far + c
    sends = [
        piece(0, me, top, to_right),
        piece(1, me, bottom, to_left),
        piece(2, me, bottom, to_right),
        piece(3, me, top, to_left),
        piece(4, me, None, to_other),
    ]
    for copy in sends:
        copy.start()
    consume(me)

    def forward(number, p, rows, device):
        copy = piece(number, p, rows, device)
        copy.start()
        sends.append(copy)

    piece(0, from_left, top, to_right).wait_recv()
    forward(5, from_left, top, to_right)
    piece(1, from_right, bottom, to_left).wait_recv()
    forward(6, from_right, bottom, to_left)
    piece(4, 2 * x + other, None, to_other).wait_recv()
    consume(2 * x + other)
    piece(2, from_left, bottom, to_right).wait_recv()
    forward(7, from_left, None, to_other)
    piece(3, from_right, top, to_left).wait_recv()
    forward(8, from_right, None, to_other)
    consume(from_left)
    consume(from_right)
    piece(5, across, top, to_right).wait_recv()
    piece(6, across, bottom, to_left).wait_recv()
    forward(9, across, None, to_other)
    piece(7, 2 * left + other, None, to_other).wait_recv()
    consume(2 * left + other)
    piece(8, 2 * right + other, None, to_other).wait_recv()
    consume(2 * right + other)
    consume(across)
    piece(9, 2 * far + other, None, to_other).wait_recv()
    consume(2 * far + other)
    for copy in sends:
        copy.wait_send()


def project_kernel(
    nx, tokens_ref, gain_ref, *refs
):
    weights, out_ref = refs[:6], refs[6]
    slots, held, total, squares, local_sem, weight_sem, send_sem, recv_sem = refs[7:]
    x, c = lax.axis_index("x"), lax.axis_index("c")
    own = pltpu.make_async_copy(tokens_ref, slots.at[2 * x + c], local_sem)
    own.start()
    width = weights[0].shape[1]
    loads = [
        pltpu.make_async_copy(ref, held.at[:, pl.ds(n * width, width)], weight_sem.at[n])
        for n, ref in enumerate(weights)
    ]
    for load in loads:
        load.start()
    total[...] = jnp.zeros_like(total)
    squares[...] = jnp.zeros_like(squares)
    tp_greet(nx)
    own.wait()
    features = tokens_ref.shape[1]
    waited = []

    def consume(p):
        if not waited:
            for load in loads:
                load.wait()
            waited.append(True)
        wide = slots[p].astype(F32)
        squared = wide * wide
        folded = squared[:, :128]
        for k in range(1, features // 128):
            folded = folded + squared[:, k * 128 : (k + 1) * 128]
        squares[...] += folded
        scaled = (wide * gain_ref[p]).astype(BF16)
        rows = pl.ds(pl.multiple_of(p * features, features), features)
        total[...] += jnp.dot(scaled, held[rows, :], preferred_element_type=F32)

    tp_gather(nx, slots, send_sem, recv_sem, consume)
    mean = jnp.sum(squares[...], axis=1, keepdims=True) / held.shape[0]
    inverse = lax.rsqrt(mean + EPSILON)
    out_ref[...] = (total[...] * inverse).astype(BF16)


def output_kernel(nx, rows_ref, recur_ref, attend_ref, out_ref, slots, held, total, local_sem, weight_sem, send_sem, recv_sem):
    x, c = lax.axis_index("x"), lax.axis_index("c")
    own = pltpu.make_async_copy(rows_ref, slots.at[2 * x + c], local_sem)
    own.start()
    depth = rows_ref.shape[1] // 2
    pieces = 2 * nx
    loads = []
    for n in range(pieces):
        for k, ref in enumerate((recur_ref, attend_ref)):
            loads.append(
                pltpu.make_async_copy(
                    ref.at[pl.ds(n * depth, depth)], held.at[n, pl.ds(k * depth, depth)], weight_sem.at[2 * n + k]
                )
            )
    for load in loads:
        load.start()
    total[...] = jnp.zeros_like(total)
    tp_greet(nx)
    own.wait()
    waited = []

    def consume(p):
        if not waited:
            for load in loads:
                load.wait()
            waited.append(True)
        total[...] += jnp.dot(slots[p], held[p], preferred_element_type=F32)

    tp_gather(nx, slots, send_sem, recv_sem, consume)
    out_ref[...] = total[...].astype(BF16)


def thirds(value):
    first = value.astype(BF16)
    rest = value - first.astype(F32)
    second = rest.astype(BF16)
    third = (rest - second.astype(F32)).astype(BF16)
    return first, second, third


def whole(first, second, third):
    return first.astype(F32) + second.astype(F32) + third.astype(F32)


def padded_thirds(rows, height):
    parts = [part.astype(F32) for row in rows for part in thirds(row)]
    parts.append(jnp.zeros((height - len(parts), rows[0].shape[1]), F32))
    return jnp.concatenate(parts, axis=0).astype(BF16)


def nt(left, right):
    return lax.dot_general(left, right, (((1,), (1,)), ((), ())), preferred_element_type=F32)


def middle_kernel(
    nz,
    ny,
    proj_ref,
    floor_ref,
    decay_ref,
    start_ref,
    recur_gain_ref,
    gate_ref,
    attend_gain_ref,
    out_ref,
    kbuf,
    vbuf,
    qbuf,
    sbuf,
    tbuf,
    obuf,
    rbuf,
    acc,
    top,
    bias,
    score_s,
    weight_s,
    top_s,
    scale_s,
    scale_w,
    kv_send,
    kv_recv,
    q_send,
    q_recv,
    t_send,
    t_recv,
    o_send,
    o_recv,
):
    z, y = lax.axis_index("z"), lax.axis_index("y")
    height = proj_ref.shape[0]
    row_at = z * ny * height

    def gates(zq, yq):
        at = pl.multiple_of((zq * ny + yq) * height, height)
        return gate_ref[:, pl.ds(at, height)]

    barrier = pltpu.get_barrier_semaphore()
    for step in (1, ny - 1):
        pl.semaphore_signal(barrier, inc=1, device_id={"y": lax.rem(y + step, ny)}, device_id_type=MESH)
    for step in range(1, nz):
        pl.semaphore_signal(barrier, inc=1, device_id={"z": lax.rem(z + step, nz)}, device_id_type=MESH)

    kbuf[y] = proj_ref[:, 512:640]
    values_t = jnp.transpose(proj_ref[:, 640:768].astype(F32))
    vbuf[y] = values_t.astype(BF16)
    query_t = jnp.transpose(proj_ref[:, 384:512].astype(F32) * (FD**-0.5))
    qbuf[z] = query_t.astype(BF16)
    pl.semaphore_wait(barrier, nz + 1)

    y_next, y_last = {"y": lax.rem(y + 1, ny)}, {"y": lax.rem(y + ny - 1, ny)}
    z_next, z_last = {"z": lax.rem(z + 1, nz)}, {"z": lax.rem(z + nz - 1, nz)}
    kv = (kbuf, vbuf, sbuf)

    def y_copy(way, unit, slot, step):
        device = y_next if way == 0 else y_last
        ref = kv[unit].at[slot]
        return remote(ref, ref, kv_send.at[way, unit, step], kv_recv.at[way, unit, step], device)

    def z_copy(way, slot, step):
        device = z_next if way == 0 else z_last
        ref = qbuf.at[slot]
        return remote(ref, ref, q_send.at[way, step], q_recv.at[way, step], device)

    def y_units(way, step):
        if 2 * step < ny:
            return (0, 1, 2)
        return (0, 2) if way == 0 else (1,)

    def y_slot(way, step):
        return lax.rem(y + ny - step, ny) if way == 0 else lax.rem(y + step, ny)

    def z_slot(way, step):
        return lax.rem(z + nz - step, nz) if way == 0 else lax.rem(z + step, nz)

    started = []

    def begin(copy):
        copy.start()
        started.append(copy)

    def y_begin(step, units):
        for unit in units:
            for way in (0, 1):
                if unit in y_units(way, step):
                    begin(y_copy(way, unit, y_slot(way, step - 1), step - 1))

    def z_ways(step):
        return (0, 1) if 2 * step < nz else (0,)

    y_begin(1, (0, 1))
    for way in z_ways(1):
        begin(z_copy(way, z, 0))

    queries = proj_ref[:, 0:128].astype(F32)
    forget = proj_ref[:, 128:256].astype(F32)
    values = proj_ref[:, 256:384]
    inflow = (1.0 - floor_ref[...]) / (1.0 + jnp.exp(forget))
    extra = jnp.transpose(jnp.broadcast_to(decay_ref[...], (128, height)))
    decays = jnp.log1p(-inflow) - extra
    rows_i = lax.broadcasted_iota(jnp.int32, (height, height), 0)
    cols_i = lax.broadcasted_iota(jnp.int32, (height, height), 1)
    lower = jnp.where(cols_i <= rows_i, 1.0, 0.0).astype(BF16)
    sums = jnp.zeros((height, 128), F32)
    for part in thirds(decays):
        sums = sums + jnp.dot(lower, part, preferred_element_type=F32)
    ending = sums[height - 1 : height, :]
    kept = (inflow * jnp.exp(ending - sums)).astype(BF16)
    values_rt = jnp.transpose(values.astype(F32)).astype(BF16)
    sbuf[y] = jnp.concatenate(
        [jnp.dot(values_rt, kept, preferred_element_type=F32).astype(BF16), padded_thirds([ending], 16)], axis=0
    )
    y_begin(1, (2,))
    mixing = []
    for at in range(0, height, SUB):
        reach = 128 if at + SUB <= 128 else height
        base = sums[at - 1 : at, :] if at else jnp.zeros((1, 128), F32)
        near = queries[at : at + SUB] * jnp.exp(sums[at : at + SUB] - base)
        past = inflow[:reach] * jnp.exp(jnp.minimum(base - sums[:reach], 60.0))
        piece = nt(near.astype(BF16), past.astype(BF16))
        if reach < height:
            piece = jnp.concatenate([piece, jnp.zeros((SUB, height - reach), F32)], axis=1)
        mixing.append(piece)
    mixing = jnp.where(cols_i <= rows_i, jnp.concatenate(mixing, axis=0), 0.0)
    local_out = jnp.dot(mixing.astype(BF16), values, preferred_element_type=F32)
    carried_query = (queries * jnp.exp(sums)).astype(BF16)

    reference_gate = gates(z, ny - 1)[:, height - 1 : height]
    for slot in range(ny):
        relative = reference_gate - gates(z, slot)
        for head in range(2):
            bias[slot, head] = jnp.transpose(jnp.broadcast_to(relative[head : head + 1], (128, height)))
    top[...] = jnp.full(top.shape, LOW, F32)
    acc[...] = jnp.zeros_like(acc)
    ones = jnp.ones((16, height), BF16)
    blank = jnp.zeros((FD, height), BF16)

    def update(zq, yk, own):
        keys = kbuf[yk]
        for head in range(2):
            part = qbuf[zq, head * FD : (head + 1) * FD]
            split = jnp.concatenate([part, blank] if head == 0 else [blank, part], axis=0)
            scores = jnp.dot(keys, split, preferred_element_type=F32)
            shift = bias[yk, head]
            scores = scores + jnp.concatenate([shift] * (height // 128), axis=1)
            if own:
                scores = jnp.where(rows_i <= cols_i, scores, LOW)
            old = top[zq, head]
            new = jnp.maximum(old, jnp.max(scores, axis=0, keepdims=True))
            weights = jnp.exp(scores - new[0:1])
            rescale = jnp.exp(old - new)[0:1]
            top[zq, head] = new
            left = jnp.concatenate([vbuf[yk, head * FD : (head + 1) * FD], ones], axis=0)
            acc[zq, head] = acc[zq, head] * rescale + jnp.dot(
                left, weights.astype(BF16), preferred_element_type=F32
            )

    update(z, y, True)

    def pipeline(count, place):
        def at(number):
            return place(jnp.clip(number, 0, count - 1))

        def scores_of(number, lane):
            zq, yk = at(number)
            keys = kbuf[yk]
            later = jnp.where((zq == z) & (yk > y), LOW, 0.0)
            for head in range(2):
                part = qbuf[zq, head * FD : (head + 1) * FD]
                split = jnp.concatenate([part, blank] if head == 0 else [blank, part], axis=0)
                scores = jnp.dot(keys, split, preferred_element_type=F32)
                shift = bias[yk, head] + later
                scores = scores + jnp.concatenate([shift] * (height // 128), axis=1)
                old = top[zq, head]
                new = jnp.maximum(old, jnp.max(scores, axis=0, keepdims=True))
                score_s[lane, head] = scores
                top[zq, head] = new
                top_s[lane, head] = new
                scale_s[lane, head] = jnp.exp(old - new)

        def weights_of(lane):
            for head in range(2):
                weight_s[lane, head] = jnp.exp(score_s[lane, head] - top_s[lane, head][0:1]).astype(BF16)
                scale_w[lane, head] = scale_s[lane, head]

        def sums_of(number, lane):
            zq, yk = at(number)
            for head in range(2):
                left = jnp.concatenate([vbuf[yk, head * FD : (head + 1) * FD], ones], axis=0)
                acc[zq, head] = acc[zq, head] * scale_w[lane, head][0:1] + jnp.dot(
                    left, weight_s[lane, head], preferred_element_type=F32
                )

        weight_s[...] = jnp.zeros_like(weight_s)
        scale_w[...] = jnp.ones_like(scale_w)
        for lane in range(LANES):
            scores_of(lane, lane)
        rounds = (count + LANES - 1) // LANES

        def turn(n, carry):
            for lane in range(LANES):
                number = n * LANES + lane
                sums_of(number - LANES, lane)
                weights_of(lane)
                scores_of(number + LANES, lane)
            return carry

        lax.fori_loop(0, rounds, turn, 0)
        for lane in range(LANES):
            number = (rounds - 1) * LANES + lane

            @pl.when(number < count)
            def _(number=number, lane=lane):
                sums_of(number, lane)

    def fold(step):
        last = 2 * step == nz
        back = min(step, nz // 2 - 1)
        ahead = jnp.minimum(step, nz - 1 - z) + 1
        behind = jnp.maximum(back - z, 0)
        fresh = 1 if last else 2
        first = (ahead + behind) * fresh
        one = jnp.where(z + step <= nz - 1, 1, 0)
        two = 0 if last else jnp.where(z <= step - 1, 1, 0)
        known = 2 * step - 1

        def place(number):
            which = number // fresh
            oq = jnp.where(which < ahead, which, nz - back + which - ahead)
            ok = step if last else (number % 2) * (2 * step) - step
            rest = jnp.maximum(number - first, 0)
            second = rest // known
            oq_new = jnp.where((second == 0) & (one == 1), step, nz - step)
            ok_new = rest % known - (step - 1)
            old = number < first
            return z + jnp.where(old, oq, oq_new), lax.rem(y + jnp.where(old, ok, ok_new) + ny, ny)

        pipeline(first + (one + two) * known, place)

    for step in range(1, ny // 2 + 1):
        for unit in (0, 1, 2):
            for way in (0, 1):
                if unit in y_units(way, step):
                    slot = y_slot(way, step)
                    y_copy(way, unit, slot, step - 1).wait_recv()
                    if unit in y_units(way, step + 1) and step < ny // 2:
                        begin(y_copy(way, unit, slot, step))
        for way in z_ways(step):
            slot = z_slot(way, step)
            z_copy(way, slot, step - 1).wait_recv()
            if step < nz // 2 and way in z_ways(step + 1):
                begin(z_copy(way, slot, step))
        if step < ny // 2:
            fold(step)
        else:
            state = jnp.zeros((128, 128), F32)
            inside = state
            log_all = jnp.zeros((1, 128), F32)
            log_before = log_all
            for slot in range(ny):
                block = sbuf[slot].astype(F32)
                log_own = block[128:129] + block[129:130] + block[130:131]
                state = state * jnp.exp(log_own) + block[:128]
                log_all = log_all + log_own
                inside = jnp.where(slot < y, state, inside)
                log_before = jnp.where(slot < y, log_all, log_before)
            tbuf[z] = jnp.concatenate([state.astype(BF16), padded_thirds([log_all], 16)], axis=0)

            def t_copy(slot, target):
                ref = tbuf.at[slot]
                return remote(ref, ref, t_send.at[target], t_recv.at[slot], {"z": target})

            @pl.loop(z + 1, nz)
            def _(target):
                t_copy(z, target).start()

            fold(step)

    def o_copy(source, slot, target):
        return remote(obuf.at[slot], rbuf.at[source], o_send.at[slot], o_recv.at[source], {"z": target})

    def logs_of(zq):
        shift = gates(zq, y) - reference_gate
        return [
            top[zq, head][0:1] + jnp.log(acc[zq, head][FD : FD + 1]) + shift[head : head + 1] for head in range(2)
        ]

    def rows_of(zq):
        return [acc[zq, head][:FD] / acc[zq, head][FD : FD + 1] for head in range(2)]

    @pl.loop(z + 1, nz)
    def _(target):
        obuf[target] = jnp.concatenate(
            [part.astype(BF16) for part in rows_of(target)] + [padded_thirds(logs_of(target), 16)], axis=0
        )
        o_copy(z, target, target).start()

    def take(slot, state):
        t_copy(slot, z).wait_recv()
        block = tbuf[slot].astype(F32)
        log_own = block[128:129] + block[129:130] + block[130:131]
        return state * jnp.exp(log_own) + block[:128]

    arriving = lax.fori_loop(0, z, take, jnp.transpose(start_ref[...]))
    arriving = arriving * jnp.exp(log_before) + inside
    rec_out = local_out + nt(carried_query, arriving.astype(BF16))
    mean = jnp.mean(rec_out * rec_out, axis=1, keepdims=True)
    out_ref[:, 0:128] = (rec_out * lax.rsqrt(mean + EPSILON) * recur_gain_ref[...]).astype(BF16)

    def merge(slot, carry):
        o_copy(slot, slot, z).wait_recv()
        block = rbuf[slot].astype(F32)
        merged = []
        for head in range(2):
            best, amount, rows = carry[3 * head : 3 * head + 3]
            at = 2 * FD + 3 * head
            log = block[at : at + 1] + block[at + 1 : at + 2] + block[at + 2 : at + 3]
            new = jnp.maximum(best, log)
            keep, add = jnp.exp(best - new), jnp.exp(log - new)
            merged += [new, amount * keep + add, rows * keep + block[head * FD : (head + 1) * FD] * add]
        return tuple(merged)

    own_logs, own_rows = logs_of(z), rows_of(z)
    start = []
    for head in range(2):
        start += [own_logs[head], jnp.ones((1, height), F32), own_rows[head]]
    merged = lax.fori_loop(0, z, merge, tuple(start))
    normed = []
    for head in range(2):
        rows = merged[3 * head + 2] / merged[3 * head + 1]
        mean = jnp.mean(rows * rows, axis=0, keepdims=True)
        normed.append(rows * lax.rsqrt(mean + EPSILON))
    att_rows = jnp.transpose(jnp.concatenate(normed, axis=0))
    out_ref[:, 128:256] = (att_rows * attend_gain_ref[...]).astype(BF16)

    for copy in started:
        copy.wait_send()

    @pl.loop(z + 1, nz)
    def _(target):
        t_copy(z, target).wait_send()
        o_copy(z, target, target).wait_send()


VM = pl.BlockSpec(memory_space=pltpu.VMEM)
ANY = pl.BlockSpec(memory_space=pl.ANY)
DMA = pltpu.SemaphoreType.DMA


def params(number):
    return pltpu.CompilerParams(collective_id=number, has_side_effects=True, vmem_limit_bytes=VMEM_LIMIT)


def project(nx, tokens, norm_gain, weights):
    height, features = tokens.shape
    model = norm_gain.shape[0]
    width = sum(weight.shape[1] for weight in weights)
    return pl.pallas_call(
        functools.partial(project_kernel, nx),
        out_shape=jax.ShapeDtypeStruct((height, width), BF16),
        in_specs=[ANY, VM] + [ANY] * 6,
        out_specs=VM,
        scratch_shapes=[
            pltpu.VMEM((2 * nx, height, features), BF16),
            pltpu.VMEM((model, width), BF16),
            pltpu.VMEM((height, width), F32),
            pltpu.VMEM((height, 128), F32),
            DMA,
            DMA((6,)),
            DMA((10,)),
            DMA((10,)),
        ],
        compiler_params=params(0),
        name="project",
    )(tokens, norm_gain.reshape(2 * nx, 1, features), *weights)


def middle(nz, ny, projected, gate_floor, extra_decay, start_state, recur_gain, gate_cache, attend_gain):
    height = projected.shape[0]
    return pl.pallas_call(
        functools.partial(middle_kernel, nz, ny),
        out_shape=jax.ShapeDtypeStruct((height, 256), BF16),
        in_specs=[VM] * 7,
        out_specs=VM,
        scratch_shapes=[
            pltpu.VMEM((ny, height, 128), BF16),
            pltpu.VMEM((ny, 128, height), BF16),
            pltpu.VMEM((nz, 128, height), BF16),
            pltpu.VMEM((ny, 144, 128), BF16),
            pltpu.VMEM((nz, 144, 128), BF16),
            pltpu.VMEM((nz, 144, height), BF16),
            pltpu.VMEM((nz, 144, height), BF16),
            pltpu.VMEM((nz, 2, FD + 16, height), F32),
            pltpu.VMEM((nz, 2, 8, height), F32),
            pltpu.VMEM((ny, 2, height, 128), F32),
            pltpu.VMEM((LANES, 2, height, height), F32),
            pltpu.VMEM((LANES, 2, height, height), BF16),
            pltpu.VMEM((LANES, 2, 8, height), F32),
            pltpu.VMEM((LANES, 2, 8, height), F32),
            pltpu.VMEM((LANES, 2, 8, height), F32),
            DMA((2, 3, ny // 2)),
            DMA((2, 3, ny // 2)),
            DMA((2, nz // 2)),
            DMA((2, nz // 2)),
            DMA((nz,)),
            DMA((nz,)),
            DMA((nz,)),
            DMA((nz,)),
        ],
        compiler_params=params(1),
        name="middle",
    )(
        projected,
        gate_floor.reshape(1, -1),
        extra_decay.reshape(1, -1),
        start_state.reshape(128, 128),
        recur_gain.reshape(1, -1),
        gate_cache.T,
        attend_gain.reshape(1, -1),
    )


def output(nx, rows, recur_output, attend_output):
    height = rows.shape[0]
    width = recur_output.shape[1]
    return pl.pallas_call(
        functools.partial(output_kernel, nx),
        out_shape=jax.ShapeDtypeStruct((height, width), BF16),
        in_specs=[ANY] * 3,
        out_specs=VM,
        scratch_shapes=[
            pltpu.VMEM((2 * nx, height, 256), BF16),
            pltpu.VMEM((2 * nx, 256, width), BF16),
            pltpu.VMEM((height, width), F32),
            DMA,
            DMA((4 * nx,)),
            DMA((10,)),
            DMA((10,)),
        ],
        compiler_params=params(2),
        name="output",
    )(rows, recur_output, attend_output)


def shards(
    sizes,
    tokens,
    norm_gain,
    recur_query,
    recur_forget,
    recur_value,
    gate_floor,
    extra_decay,
    start_state,
    recur_gain,
    attend_query,
    attend_key,
    attend_value,
    gate_cache,
    attend_gain,
    recur_output,
    attend_output,
):
    nz, ny, nx = sizes
    weights = (recur_query, recur_forget, recur_value, attend_query, attend_key, attend_value)
    projected = project(nx, tokens, norm_gain, weights)
    rows = middle(nz, ny, projected, gate_floor, extra_decay, start_state, recur_gain, gate_cache, attend_gain)
    return output(nx, rows, recur_output, attend_output)


def solution(mesh):
    sizes = (8, 8, 4)
    finer = Mesh(mesh.devices.reshape(*sizes, 2), ("z", "y", "x", "c"))
    return jax.shard_map(
        functools.partial(shards, sizes),
        mesh=finer,
        in_specs=(
            P(SP, TP),
            P(),
            P(None, TP),
            P(None, TP),
            P(None, TP),
            P(TP),
            P(SP, TP),
            P(TP, None, None),
            P(TP),
            P(None, TP),
            P(None, TP),
            P(None, TP),
            P(None, TP),
            P(TP),
            P(None, TP),
            P(None, TP),
        ),
        out_specs=P(SP, TP),
        check_vma=False,
    )
```

```python
import functools

import jax
import jax.numpy as jnp
from jax import lax
from jax.experimental import pallas as pl
from jax.experimental.pallas import tpu as pltpu
from jax.sharding import Mesh
from jax.sharding import PartitionSpec as P

FD = 64
SP = ("z", "y")
TP = ("x", "c")
EPSILON = 1e-06
LOW = -1e30
SUB = 16
LANES = 2
F32 = jnp.float32
BF16 = jnp.bfloat16
MESH = pl.DeviceIdType.MESH
VMEM_LIMIT = 60 * 1024 * 1024


def remote(src, dst, send, recv, device):
    return pltpu.make_async_remote_copy(
        src_ref=src, dst_ref=dst, send_sem=send, recv_sem=recv, device_id=device, device_id_type=MESH
    )


def tp_greet(nx):
    x, c = lax.axis_index("x"), lax.axis_index("c")
    barrier = pltpu.get_barrier_semaphore()
    peers = [{"c": 1 - c}, {"x": lax.rem(x + 1, nx)}, {"x": lax.rem(x + nx - 1, nx)}]
    for peer in peers:
        pl.semaphore_signal(barrier, inc=1, device_id=peer, device_id_type=MESH)
    pl.semaphore_wait(barrier, len(peers))


def tp_gather(nx, slots, send_sem, recv_sem, consume):
    x, c = lax.axis_index("x"), lax.axis_index("c")
    other = 1 - c
    right, left, far = lax.rem(x + 1, nx), lax.rem(x + nx - 1, nx), lax.rem(x + 2, nx)
    half = slots.shape[1] // 2
    me = 2 * x + c
    top, bottom = pl.ds(0, half), pl.ds(half, half)

    def piece(number, p, rows, device):
        ref = slots.at[p] if rows is None else slots.at[p, rows]
        return remote(ref, ref, send_sem.at[number], recv_sem.at[number], device)

    to_right, to_left, to_other = {"x": right}, {"x": left}, {"c": other}
    from_left, from_right, across = 2 * left + c, 2 * right + c, 2 * far + c
    sends = [
        piece(0, me, top, to_right),
        piece(1, me, bottom, to_left),
        piece(2, me, bottom, to_right),
        piece(3, me, top, to_left),
        piece(4, me, None, to_other),
    ]
    for copy in sends:
        copy.start()
    consume(me)

    def forward(number, p, rows, device):
        copy = piece(number, p, rows, device)
        copy.start()
        sends.append(copy)

    piece(0, from_left, top, to_right).wait_recv()
    forward(5, from_left, top, to_right)
    piece(1, from_right, bottom, to_left).wait_recv()
    forward(6, from_right, bottom, to_left)
    piece(4, 2 * x + other, None, to_other).wait_recv()
    consume(2 * x + other)
    piece(2, from_left, bottom, to_right).wait_recv()
    forward(7, from_left, None, to_other)
    piece(3, from_right, top, to_left).wait_recv()
    forward(8, from_right, None, to_other)
    consume(from_left)
    consume(from_right)
    piece(5, across, top, to_right).wait_recv()
    piece(6, across, bottom, to_left).wait_recv()
    forward(9, across, None, to_other)
    piece(7, 2 * left + other, None, to_other).wait_recv()
    consume(2 * left + other)
    piece(8, 2 * right + other, None, to_other).wait_recv()
    consume(2 * right + other)
    consume(across)
    piece(9, 2 * far + other, None, to_other).wait_recv()
    consume(2 * far + other)
    for copy in sends:
        copy.wait_send()


def project_kernel(
    nx, tokens_ref, gain_ref, *refs
):
    weights, out_ref = refs[:6], refs[6]
    slots, held, total, squares, local_sem, weight_sem, send_sem, recv_sem = refs[7:]
    x, c = lax.axis_index("x"), lax.axis_index("c")
    own = pltpu.make_async_copy(tokens_ref, slots.at[2 * x + c], local_sem)
    own.start()
    width = weights[0].shape[1]
    loads = [
        pltpu.make_async_copy(ref, held.at[:, pl.ds(n * width, width)], weight_sem.at[n])
        for n, ref in enumerate(weights)
    ]
    for load in loads:
        load.start()
    total[...] = jnp.zeros_like(total)
    squares[...] = jnp.zeros_like(squares)
    tp_greet(nx)
    own.wait()
    features = tokens_ref.shape[1]
    waited = []

    def consume(p):
        if not waited:
            for load in loads:
                load.wait()
            waited.append(True)
        wide = slots[p].astype(F32)
        squared = wide * wide
        folded = squared[:, :128]
        for k in range(1, features // 128):
            folded = folded + squared[:, k * 128 : (k + 1) * 128]
        squares[...] += folded
        scaled = (wide * gain_ref[p]).astype(BF16)
        rows = pl.ds(pl.multiple_of(p * features, features), features)
        total[...] += jnp.dot(scaled, held[rows, :], preferred_element_type=F32)

    tp_gather(nx, slots, send_sem, recv_sem, consume)
    mean = jnp.sum(squares[...], axis=1, keepdims=True) / held.shape[0]
    inverse = lax.rsqrt(mean + EPSILON)
    out_ref[...] = (total[...] * inverse).astype(BF16)


def output_kernel(nx, rows_ref, recur_ref, attend_ref, out_ref, slots, held, total, local_sem, weight_sem, send_sem, recv_sem):
    x, c = lax.axis_index("x"), lax.axis_index("c")
    own = pltpu.make_async_copy(rows_ref, slots.at[2 * x + c], local_sem)
    own.start()
    depth = rows_ref.shape[1] // 2
    pieces = 2 * nx
    loads = []
    for n in range(pieces):
        for k, ref in enumerate((recur_ref, attend_ref)):
            loads.append(
                pltpu.make_async_copy(
                    ref.at[pl.ds(n * depth, depth)], held.at[n, pl.ds(k * depth, depth)], weight_sem.at[2 * n + k]
                )
            )
    for load in loads:
        load.start()
    total[...] = jnp.zeros_like(total)
    tp_greet(nx)
    own.wait()
    waited = []

    def consume(p):
        if not waited:
            for load in loads:
                load.wait()
            waited.append(True)
        total[...] += jnp.dot(slots[p], held[p], preferred_element_type=F32)

    tp_gather(nx, slots, send_sem, recv_sem, consume)
    out_ref[...] = total[...].astype(BF16)


def thirds(value):
    first = value.astype(BF16)
    rest = value - first.astype(F32)
    second = rest.astype(BF16)
    third = (rest - second.astype(F32)).astype(BF16)
    return first, second, third


def whole(first, second, third):
    return first.astype(F32) + second.astype(F32) + third.astype(F32)


def padded_thirds(rows, height):
    parts = [part.astype(F32) for row in rows for part in thirds(row)]
    parts.append(jnp.zeros((height - len(parts), rows[0].shape[1]), F32))
    return jnp.concatenate(parts, axis=0).astype(BF16)


def nt(left, right):
    return lax.dot_general(left, right, (((1,), (1,)), ((), ())), preferred_element_type=F32)


def middle_kernel(
    size,
    proj_ref,
    floor_ref,
    decay_ref,
    start_ref,
    recur_gain_ref,
    gate_ref,
    attend_gain_ref,
    out_ref,
    kbuf,
    vbuf,
    qbuf,
    slice_out,
    slice_in,
    total_in,
    state_out,
    state_in,
    start_t,
    prefix,
    log_prefix,
    obuf,
    rbuf,
    acc,
    top,
    bias,
    score_s,
    weight_s,
    top_s,
    scale_s,
    scale_w,
    kv_send,
    kv_recv,
    q_send,
    q_recv,
    s_send,
    s_recv,
    t_send,
    t_recv,
    u_send,
    u_recv,
    o_send,
    o_recv,
):
    z, y, c = lax.axis_index("z"), lax.axis_index("y"), lax.axis_index("c")
    height = proj_ref.shape[0]
    mine = 1 - c
    a, b = mine * y + c * z, mine * z + c * y

    def on_a(index):
        return {"y": mine * index + c * y, "z": mine * z + c * index}

    def on_b(index):
        return {"z": mine * index + c * z, "y": mine * y + c * index}

    def gates(block):
        return gate_ref[:, pl.ds(pl.multiple_of(block * height, height), height)]

    def key_gates(index):
        return gates(mine * (z * size + index) + c * (index * size + y))

    def query_gates(index):
        return gates(mine * (index * size + y) + c * (z * size + index))

    def shifted(place, offset):
        return lax.rem(place + offset + size, size)

    barrier = pltpu.get_barrier_semaphore()
    for step in range(1, size):
        for device in ({"y": shifted(y, step)}, {"z": shifted(z, step)}):
            pl.semaphore_signal(barrier, inc=1, device_id=device, device_id_type=MESH)

    kbuf[a] = proj_ref[:, 512:640]
    values_t = jnp.transpose(proj_ref[:, 640:768].astype(F32))
    vbuf[a] = values_t.astype(BF16)
    query_t = jnp.transpose(proj_ref[:, 384:512].astype(F32) * (FD**-0.5))
    qbuf[b] = query_t.astype(BF16)
    pl.semaphore_wait(barrier, 2 * (size - 1))

    kv = (kbuf, vbuf)

    def a_copy(way, unit, slot, step):
        ref = kv[unit].at[slot]
        target = on_a(shifted(a, 1 if way == 0 else -1))
        return remote(ref, ref, kv_send.at[way, unit, step], kv_recv.at[way, unit, step], target)

    def b_copy(way, slot, step):
        ref = qbuf.at[slot]
        target = on_b(shifted(b, 1 if way == 0 else -1))
        return remote(ref, ref, q_send.at[way, step], q_recv.at[way, step], target)

    def a_units(way, step):
        if 2 * step < size:
            return (0, 1)
        return (0,) if way == 0 else (1,)

    def slot_of(place, way, step):
        return shifted(place, -step if way == 0 else step)

    def b_ways(step):
        return (0, 1) if 2 * step < size else (0,)

    started = []

    def begin(copy):
        copy.start()
        started.append(copy)

    for unit in (0, 1):
        for way in (0, 1):
            begin(a_copy(way, unit, a, 0))
    for way in (0, 1):
        begin(b_copy(way, b, 0))

    queries = proj_ref[:, 0:128].astype(F32)
    forget = proj_ref[:, 128:256].astype(F32)
    values = proj_ref[:, 256:384]
    inflow = (1.0 - floor_ref[...]) / (1.0 + jnp.exp(forget))
    extra = jnp.transpose(jnp.broadcast_to(decay_ref[...], (128, height)))
    decays = jnp.log1p(-inflow) - extra
    rows_i = lax.broadcasted_iota(jnp.int32, (height, height), 0)
    cols_i = lax.broadcasted_iota(jnp.int32, (height, height), 1)
    lower = jnp.where(cols_i <= rows_i, 1.0, 0.0).astype(BF16)
    sums = jnp.zeros((height, 128), F32)
    for third in thirds(decays):
        sums = sums + jnp.dot(lower, third, preferred_element_type=F32)
    ending = sums[height - 1 : height, :]
    kept = (inflow * jnp.exp(ending - sums)).astype(BF16)
    values_rt = jnp.transpose(values.astype(F32)).astype(BF16)
    own_state = jnp.dot(values_rt, kept, preferred_element_type=F32).astype(BF16)

    part = 128 // size
    logs = padded_thirds([ending], 16)
    for target in range(size):
        slice_out[target] = jnp.concatenate([own_state[target * part : (target + 1) * part], logs], axis=0)
    slice_in[y] = slice_out[y]
    turned = jnp.transpose(start_ref[...])
    for slot in range(size):
        start_t[slot] = turned[slot * part : (slot + 1) * part]

    def slice_copy(source, target):
        return remote(
            slice_out.at[target], slice_in.at[source], s_send.at[target], s_recv.at[source], {"y": target}
        )

    @pl.loop(1, size)
    def _(step):
        slice_copy(y, shifted(y, step)).start()

    mixing = []
    for at in range(0, height, SUB):
        reach = 128 if at + SUB <= 128 else height
        base = sums[at - 1 : at, :] if at else jnp.zeros((1, 128), F32)
        near = queries[at : at + SUB] * jnp.exp(sums[at : at + SUB] - base)
        past = inflow[:reach] * jnp.exp(jnp.minimum(base - sums[:reach], 60.0))
        piece = nt(near.astype(BF16), past.astype(BF16))
        if reach < height:
            piece = jnp.concatenate([piece, jnp.zeros((SUB, height - reach), F32)], axis=1)
        mixing.append(piece)
    mixing = jnp.where(cols_i <= rows_i, jnp.concatenate(mixing, axis=0), 0.0)
    local_out = jnp.dot(mixing.astype(BF16), values, preferred_element_type=F32)
    carried_query = (queries * jnp.exp(sums)).astype(BF16)

    reference_gate = key_gates(mine * (size - 1) + c * z)[:, height - 1 : height]
    for slot in range(size):
        relative = reference_gate - key_gates(slot)
        for head in range(2):
            bias[slot, head] = jnp.transpose(jnp.broadcast_to(relative[head : head + 1], (128, height)))
    top[...] = jnp.full(top.shape, LOW, F32)
    acc[...] = jnp.zeros_like(acc)
    ones = jnp.ones((16, height), BF16)
    blank = jnp.zeros((FD, height), BF16)

    def split_query(iq, head):
        piece = qbuf[iq, head * FD : (head + 1) * FD]
        return jnp.concatenate([piece, blank] if head == 0 else [blank, piece], axis=0)

    def with_ones(ik, head):
        return jnp.concatenate([vbuf[ik, head * FD : (head + 1) * FD], ones], axis=0)

    def wide(column):
        return jnp.concatenate([column] * (height // 128), axis=1)

    def fold_own():
        for head in range(2):
            scores = jnp.dot(kbuf[a], split_query(b, head), preferred_element_type=F32) + wide(bias[a, head])
            scores = jnp.where(rows_i <= cols_i, scores, LOW)
            new = jnp.broadcast_to(jnp.max(scores, axis=0, keepdims=True), (8, height))
            top[b, head] = new
            weights = jnp.exp(scores - new[0:1]).astype(BF16)
            acc[b, head] = jnp.dot(with_ones(a, head), weights, preferred_element_type=F32)

    fold_own()

    def pipeline(count, place):
        def at(number):
            return place(jnp.clip(number, 0, count - 1))

        def scores_of(number, lane):
            iq, ik = at(number)
            keys = kbuf[ik]
            row, column = mine * iq + c * ik, mine * ik + c * iq
            later = jnp.where((row == z) & ((column - y) * (mine - c) > 0), LOW, 0.0)
            for head in range(2):
                scores = jnp.dot(keys, split_query(iq, head), preferred_element_type=F32)
                scores = scores + wide(bias[ik, head] + later)
                old = top[iq, head]
                new = jnp.maximum(old, jnp.max(scores, axis=0, keepdims=True))
                score_s[lane, head] = scores
                top[iq, head] = new
                top_s[lane, head] = new
                scale_s[lane, head] = jnp.exp(old - new)

        def weights_of(lane):
            for head in range(2):
                weight_s[lane, head] = jnp.exp(score_s[lane, head] - top_s[lane, head][0:1]).astype(BF16)
                scale_w[lane, head] = scale_s[lane, head]

        def sums_of(number, lane):
            iq, ik = at(number)
            for head in range(2):
                acc[iq, head] = acc[iq, head] * scale_w[lane, head][0:1] + jnp.dot(
                    with_ones(ik, head), weight_s[lane, head], preferred_element_type=F32
                )

        weight_s[...] = jnp.zeros_like(weight_s)
        scale_w[...] = jnp.ones_like(scale_w)
        for lane in range(LANES):
            scores_of(lane, lane)
        rounds = (count + LANES - 1) // LANES

        def turn(n, carry):
            for lane in range(LANES):
                number = n * LANES + lane
                sums_of(number - LANES, lane)
                weights_of(lane)
                scores_of(number + LANES, lane)
            return carry

        lax.fori_loop(0, rounds, turn, 0)
        for lane in range(LANES):
            number = (rounds - 1) * LANES + lane

            @pl.when(number < count)
            def _(number=number, lane=lane):
                sums_of(number, lane)

    reach = mine * (size - 1 - z) + c * z

    def fold(step):
        last = 2 * step == size
        back = min(step, size // 2 - 1)
        ahead = jnp.minimum(step, reach) + 1
        behind = jnp.maximum(back - (size - 1 - reach), 0)
        fresh = 1 if last else 2
        first = (ahead + behind) * fresh
        one = jnp.where(step <= reach, 1, 0)
        two = 0 if last else jnp.where(size - step <= reach, 1, 0)
        known = 2 * step - 1

        def place(number):
            which = number // fresh
            bounded = jnp.where(which < ahead, which, size - back + which - ahead)
            free = step if last else (number % 2) * (2 * step) - step
            rest = jnp.maximum(number - first, 0)
            bounded_new = jnp.where((rest // known == 0) & (one == 1), step, size - step)
            free_new = rest % known - (step - 1)
            old = number < first
            bounded, free = jnp.where(old, bounded, bounded_new), jnp.where(old, free, free_new)
            iq = mine * (b + bounded) + c * shifted(b, free)
            ik = mine * shifted(a, free) + c * (a - bounded)
            return iq, ik

        pipeline(first + (one + two) * known, place)

    def log_of(block):
        return block[part : part + 1] + block[part + 1 : part + 2] + block[part + 2 : part + 3]

    def total_copy(source, target):
        ref = total_in.at[source]
        return remote(ref, ref, t_send.at[target], t_recv.at[source], {"z": target})

    def state_copy(source, target):
        return remote(state_out.at[target], state_in.at[source], u_send.at[target], u_recv.at[source], {"y": target})

    def row_states():
        @pl.loop(1, size)
        def _(step):
            source = shifted(y, -step)
            slice_copy(source, y).wait_recv()

        state = jnp.zeros((part, 128), F32)
        log_all = jnp.zeros((1, 128), F32)
        for slot in range(size):
            prefix[slot] = state
            log_prefix[slot] = jnp.broadcast_to(log_all, (8, 128))
            block = slice_in[slot].astype(F32)
            log_own = log_of(block)
            state = state * jnp.exp(log_own) + block[:part]
            log_all = log_all + log_own
        total_in[z] = jnp.concatenate([state.astype(BF16), padded_thirds([log_all], 16)], axis=0)

        @pl.loop(z + 1, size)
        def _(target):
            total_copy(z, target).start()

    def all_states():
        def take(slot, state):
            total_copy(slot, z).wait_recv()
            block = total_in[slot].astype(F32)
            return state * jnp.exp(log_of(block)) + block[:part]

        incoming = lax.fori_loop(0, z, take, start_t[y])
        for slot in range(size):
            state = incoming * jnp.exp(log_prefix[slot][0:1]) + prefix[slot]
            state_out[slot] = state.astype(BF16)
        state_in[y] = state_out[y]

        @pl.loop(1, size)
        def _(step):
            state_copy(y, shifted(y, step)).start()

    for step in range(1, size // 2 + 1):
        for unit in (0, 1):
            for way in (0, 1):
                if unit in a_units(way, step):
                    slot = slot_of(a, way, step)
                    a_copy(way, unit, slot, step - 1).wait_recv()
                    if 2 * step < size and unit in a_units(way, step + 1):
                        begin(a_copy(way, unit, slot, step))
        for way in b_ways(step):
            slot = slot_of(b, way, step)
            b_copy(way, slot, step - 1).wait_recv()
            if 2 * step < size and way in b_ways(step + 1):
                begin(b_copy(way, slot, step))
        fold(step)
        if step == 1:
            row_states()
        if step == 2:
            all_states()

    def o_copy(source, slot, target):
        return remote(obuf.at[slot], rbuf.at[source], o_send.at[slot], o_recv.at[source], on_b(target))

    def logs_of(iq):
        shift = query_gates(iq) - reference_gate
        return [
            top[iq, head][0:1] + jnp.log(acc[iq, head][FD : FD + 1]) + shift[head : head + 1] for head in range(2)
        ]

    def rows_of(iq):
        return [acc[iq, head][:FD] / acc[iq, head][FD : FD + 1] for head in range(2)]

    sent = mine * (size - 1 - z) + c * (size - 1)
    received = mine * z + c * (size - 1)

    @pl.loop(1, sent + 1)
    def _(step):
        target = shifted(b, step)
        obuf[target] = jnp.concatenate(
            [piece.astype(BF16) for piece in rows_of(target)] + [padded_thirds(logs_of(target), 16)], axis=0
        )
        o_copy(b, target, target).start()

    @pl.loop(1, size)
    def _(step):
        source = shifted(y, -step)
        state_copy(source, y).wait_recv()

    arriving = jnp.concatenate([state_in[slot] for slot in range(size)], axis=0)
    rec_out = local_out + nt(carried_query, arriving)
    mean = jnp.mean(rec_out * rec_out, axis=1, keepdims=True)
    out_ref[:, 0:128] = (rec_out * lax.rsqrt(mean + EPSILON) * recur_gain_ref[...]).astype(BF16)

    def merge(step, carry):
        slot = shifted(b, -step)
        o_copy(slot, slot, b).wait_recv()
        block = rbuf[slot].astype(F32)
        merged = []
        for head in range(2):
            best, amount, rows = carry[3 * head : 3 * head + 3]
            at = 2 * FD + 3 * head
            log = block[at : at + 1] + block[at + 1 : at + 2] + block[at + 2 : at + 3]
            new = jnp.maximum(best, log)
            keep, add = jnp.exp(best - new), jnp.exp(log - new)
            merged += [new, amount * keep + add, rows * keep + block[head * FD : (head + 1) * FD] * add]
        return tuple(merged)

    own_logs, own_rows = logs_of(b), rows_of(b)
    start = []
    for head in range(2):
        start += [own_logs[head], jnp.ones((1, height), F32), own_rows[head]]
    merged = lax.fori_loop(1, received + 1, merge, tuple(start))
    normed = []
    for head in range(2):
        rows = merged[3 * head + 2] / merged[3 * head + 1]
        mean = jnp.mean(rows * rows, axis=0, keepdims=True)
        normed.append(rows * lax.rsqrt(mean + EPSILON))
    att_rows = jnp.transpose(jnp.concatenate(normed, axis=0))
    out_ref[:, 128:256] = (att_rows * attend_gain_ref[...]).astype(BF16)

    for copy in started:
        copy.wait_send()

    @pl.loop(1, size)
    def _(step):
        slice_copy(y, shifted(y, step)).wait_send()
        state_copy(y, shifted(y, step)).wait_send()

    @pl.loop(z + 1, size)
    def _(target):
        total_copy(z, target).wait_send()

    @pl.loop(1, sent + 1)
    def _(step):
        target = shifted(b, step)
        o_copy(b, target, target).wait_send()


VM = pl.BlockSpec(memory_space=pltpu.VMEM)
ANY = pl.BlockSpec(memory_space=pl.ANY)
DMA = pltpu.SemaphoreType.DMA


def params(number):
    return pltpu.CompilerParams(collective_id=number, has_side_effects=True, vmem_limit_bytes=VMEM_LIMIT)


def project(nx, tokens, norm_gain, weights):
    height, features = tokens.shape
    model = norm_gain.shape[0]
    width = sum(weight.shape[1] for weight in weights)
    return pl.pallas_call(
        functools.partial(project_kernel, nx),
        out_shape=jax.ShapeDtypeStruct((height, width), BF16),
        in_specs=[ANY, VM] + [ANY] * 6,
        out_specs=VM,
        scratch_shapes=[
            pltpu.VMEM((2 * nx, height, features), BF16),
            pltpu.VMEM((model, width), BF16),
            pltpu.VMEM((height, width), F32),
            pltpu.VMEM((height, 128), F32),
            DMA,
            DMA((6,)),
            DMA((10,)),
            DMA((10,)),
        ],
        compiler_params=params(0),
        name="project",
    )(tokens, norm_gain.reshape(2 * nx, 1, features), *weights)


def middle(size, projected, gate_floor, extra_decay, start_state, recur_gain, gate_cache, attend_gain):
    height = projected.shape[0]
    part = 128 // size
    return pl.pallas_call(
        functools.partial(middle_kernel, size),
        out_shape=jax.ShapeDtypeStruct((height, 256), BF16),
        in_specs=[VM] * 7,
        out_specs=VM,
        scratch_shapes=[
            pltpu.VMEM((size, height, 128), BF16),
            pltpu.VMEM((size, 128, height), BF16),
            pltpu.VMEM((size, 128, height), BF16),
            pltpu.VMEM((size, part + 16, 128), BF16),
            pltpu.VMEM((size, part + 16, 128), BF16),
            pltpu.VMEM((size, part + 16, 128), BF16),
            pltpu.VMEM((size, part, 128), BF16),
            pltpu.VMEM((size, part, 128), BF16),
            pltpu.VMEM((size, part, 128), F32),
            pltpu.VMEM((size, part, 128), F32),
            pltpu.VMEM((size, 8, 128), F32),
            pltpu.VMEM((size, 144, height), BF16),
            pltpu.VMEM((size, 144, height), BF16),
            pltpu.VMEM((size, 2, FD + 16, height), F32),
            pltpu.VMEM((size, 2, 8, height), F32),
            pltpu.VMEM((size, 2, height, 128), F32),
            pltpu.VMEM((LANES, 2, height, height), F32),
            pltpu.VMEM((LANES, 2, height, height), BF16),
            pltpu.VMEM((LANES, 2, 8, height), F32),
            pltpu.VMEM((LANES, 2, 8, height), F32),
            pltpu.VMEM((LANES, 2, 8, height), F32),
            DMA((2, 2, size // 2)),
            DMA((2, 2, size // 2)),
            DMA((2, size // 2)),
            DMA((2, size // 2)),
        ]
        + [DMA((size,))] * 8,
        compiler_params=params(1),
        name="middle",
    )(
        projected,
        gate_floor.reshape(1, -1),
        extra_decay.reshape(1, -1),
        start_state.reshape(128, 128),
        recur_gain.reshape(1, -1),
        gate_cache.T,
        attend_gain.reshape(1, -1),
    )


def output(nx, rows, recur_output, attend_output):
    height = rows.shape[0]
    width = recur_output.shape[1]
    return pl.pallas_call(
        functools.partial(output_kernel, nx),
        out_shape=jax.ShapeDtypeStruct((height, width), BF16),
        in_specs=[ANY] * 3,
        out_specs=VM,
        scratch_shapes=[
            pltpu.VMEM((2 * nx, height, 256), BF16),
            pltpu.VMEM((2 * nx, 256, width), BF16),
            pltpu.VMEM((height, width), F32),
            DMA,
            DMA((4 * nx,)),
            DMA((10,)),
            DMA((10,)),
        ],
        compiler_params=params(2),
        name="output",
    )(rows, recur_output, attend_output)


def shards(
    sizes,
    tokens,
    norm_gain,
    recur_query,
    recur_forget,
    recur_value,
    gate_floor,
    extra_decay,
    start_state,
    recur_gain,
    attend_query,
    attend_key,
    attend_value,
    gate_cache,
    attend_gain,
    recur_output,
    attend_output,
):
    _, ny, nx = sizes
    weights = (recur_query, recur_forget, recur_value, attend_query, attend_key, attend_value)
    projected = project(nx, tokens, norm_gain, weights)
    rows = middle(ny, projected, gate_floor, extra_decay, start_state, recur_gain, gate_cache, attend_gain)
    return output(nx, rows, recur_output, attend_output)


def solution(mesh):
    sizes = (8, 8, 4)
    finer = Mesh(mesh.devices.reshape(*sizes, 2), ("z", "y", "x", "c"))
    return jax.shard_map(
        functools.partial(shards, sizes),
        mesh=finer,
        in_specs=(
            P(SP, TP),
            P(),
            P(None, TP),
            P(None, TP),
            P(None, TP),
            P(TP),
            P(SP, TP),
            P(TP, None, None),
            P(TP),
            P(None, TP),
            P(None, TP),
            P(None, TP),
            P(None, TP),
            P(TP),
            P(None, TP),
            P(None, TP),
        ),
        out_specs=P(SP, TP),
        check_vma=False,
    )
```

```python
import functools

import jax
import jax.numpy as jnp
from jax import lax
from jax.experimental import pallas as pl
from jax.experimental.pallas import tpu as pltpu
from jax.sharding import Mesh
from jax.sharding import PartitionSpec as P

FD = 64
SP = ("z", "y")
TP = ("x", "c")
EPSILON = 1e-06
LOW = -1e30
SUB = 16
LANES = 2
F32 = jnp.float32
BF16 = jnp.bfloat16
MESH = pl.DeviceIdType.MESH
VMEM_LIMIT = 60 * 1024 * 1024


def remote(src, dst, send, recv, device):
    return pltpu.make_async_remote_copy(
        src_ref=src, dst_ref=dst, send_sem=send, recv_sem=recv, device_id=device, device_id_type=MESH
    )


def tp_gather(nx, slots, send_sem, recv_sem, consume, pause=lambda: None):
    x, c = lax.axis_index("x"), lax.axis_index("c")
    other = 1 - c
    right, left, far = lax.rem(x + 1, nx), lax.rem(x + nx - 1, nx), lax.rem(x + 2, nx)
    half = slots.shape[1] // 2
    me = 2 * x + c
    top, bottom = pl.ds(0, half), pl.ds(half, half)

    def piece(number, p, rows, device):
        ref = slots.at[p] if rows is None else slots.at[p, rows]
        return remote(ref, ref, send_sem.at[number], recv_sem.at[number], device)

    to_right, to_left, to_other = {"x": right}, {"x": left}, {"c": other}
    from_left, from_right, across = 2 * left + c, 2 * right + c, 2 * far + c
    sends = [
        piece(0, me, top, to_right),
        piece(1, me, bottom, to_left),
        piece(2, me, bottom, to_right),
        piece(3, me, top, to_left),
        piece(4, me, None, to_other),
    ]
    for copy in sends:
        copy.start()
    consume(me)

    def forward(number, p, rows, device):
        copy = piece(number, p, rows, device)
        copy.start()
        sends.append(copy)

    piece(0, from_left, top, to_right).wait_recv()
    forward(5, from_left, top, to_right)
    piece(1, from_right, bottom, to_left).wait_recv()
    forward(6, from_right, bottom, to_left)
    pause()
    piece(4, 2 * x + other, None, to_other).wait_recv()
    consume(2 * x + other)
    piece(2, from_left, bottom, to_right).wait_recv()
    forward(7, from_left, None, to_other)
    piece(3, from_right, top, to_left).wait_recv()
    forward(8, from_right, None, to_other)
    pause()
    consume(from_left)
    consume(from_right)
    piece(5, across, top, to_right).wait_recv()
    piece(6, across, bottom, to_left).wait_recv()
    forward(9, across, None, to_other)
    pause()
    piece(7, 2 * left + other, None, to_other).wait_recv()
    consume(2 * left + other)
    piece(8, 2 * right + other, None, to_other).wait_recv()
    consume(2 * right + other)
    consume(across)
    piece(9, 2 * far + other, None, to_other).wait_recv()
    consume(2 * far + other)
    for copy in sends:
        copy.wait_send()


def thirds(value):
    first = value.astype(BF16)
    rest = value - first.astype(F32)
    second = rest.astype(BF16)
    third = (rest - second.astype(F32)).astype(BF16)
    return first, second, third


def whole(first, second, third):
    return first.astype(F32) + second.astype(F32) + third.astype(F32)


def padded_thirds(rows, height):
    parts = [part.astype(F32) for row in rows for part in thirds(row)]
    parts.append(jnp.zeros((height - len(parts), rows[0].shape[1]), F32))
    return jnp.concatenate(parts, axis=0).astype(BF16)


def nt(left, right):
    return lax.dot_general(left, right, (((1,), (1,)), ((), ())), preferred_element_type=F32)


def layer_kernel(
    size,
    nx,
    tokens_ref,
    gain_ref,
    weight_refs,
    floor_ref,
    decay_ref,
    start_ref,
    recur_gain_ref,
    gate_ref,
    attend_gain_ref,
    recur_output_ref,
    attend_output_ref,
    out_ref,
    slots,
    held,
    total,
    squares,
    rows_slots,
    held_out,
    local_sem,
    weight_sem,
    output_sem,
    token_send,
    token_recv,
    rows_send,
    rows_recv,
    chain,
    kbuf,
    vbuf,
    qbuf,
    slice_out,
    slice_in,
    total_in,
    state_out,
    state_in,
    start_t,
    prefix,
    log_prefix,
    obuf,
    rbuf,
    acc,
    top,
    bias,
    score_s,
    weight_s,
    top_s,
    scale_s,
    scale_w,
    kv_send,
    kv_recv,
    q_send,
    q_recv,
    s_send,
    s_recv,
    t_send,
    t_recv,
    u_send,
    u_recv,
    o_send,
    o_recv,
):
    z, y, x, c = (lax.axis_index(name) for name in ("z", "y", "x", "c"))
    height, features = tokens_ref.shape
    me = 2 * x + c

    def shifted(place, offset):
        return lax.rem(place + offset + size, size)

    own = pltpu.make_async_copy(tokens_ref, slots.at[me], local_sem)
    own.start()
    width = weight_refs[0].shape[1]
    loads = [
        pltpu.make_async_copy(ref, held.at[:, pl.ds(n * width, width)], weight_sem.at[n])
        for n, ref in enumerate(weight_refs)
    ]
    depth = recur_output_ref.shape[0] // (2 * nx)
    output_loads = [
        pltpu.make_async_copy(
            ref.at[pl.ds(n * depth, depth)], held_out.at[n, pl.ds(k * depth, depth)], output_sem.at[2 * n + k]
        )
        for n in range(2 * nx)
        for k, ref in enumerate((recur_output_ref, attend_output_ref))
    ]
    for load in loads + output_loads:
        load.start()

    barrier = pltpu.get_barrier_semaphore()
    along = [{"y": shifted(y, 1)}, {"y": shifted(y, -1)}, {"z": shifted(z, 1)}, {"z": shifted(z, -1)}]
    for device in along + [{"c": 1 - c}, {"x": lax.rem(x + 1, nx)}, {"x": lax.rem(x + nx - 1, nx)}]:
        pl.semaphore_signal(barrier, inc=1, device_id=device, device_id_type=MESH)

    def pass_on():
        for number, device in enumerate(along):
            pl.semaphore_signal(chain.at[number], inc=1, device_id=device, device_id_type=MESH)

    def hear():
        for number in range(4):
            pl.semaphore_wait(chain.at[number], 1)

    total[...] = jnp.zeros_like(total)
    squares[...] = jnp.zeros_like(squares)

    mine = 1 - c
    a, b = mine * y + c * z, mine * z + c * y

    def on_a(index):
        return {"y": mine * index + c * y, "z": mine * z + c * index}

    def on_b(index):
        return {"z": mine * index + c * z, "y": mine * y + c * index}

    def gates(block):
        return gate_ref[:, pl.ds(pl.multiple_of(block * height, height), height)]

    def key_gates(index):
        return gates(mine * (z * size + index) + c * (index * size + y))

    def query_gates(index):
        return gates(mine * (index * size + y) + c * (z * size + index))

    reference_gate = key_gates(mine * (size - 1) + c * z)[:, height - 1 : height]
    for slot in range(size):
        relative = reference_gate - key_gates(slot)
        for head in range(2):
            bias[slot, head] = jnp.transpose(jnp.broadcast_to(relative[head : head + 1], (128, height)))
    top[...] = jnp.full(top.shape, LOW, F32)
    acc[...] = jnp.zeros_like(acc)
    pl.semaphore_wait(barrier, 7)
    pass_on()
    own.wait()
    waited = []
    rounds_left = [True, True, False]

    def pause():
        hear()
        if rounds_left.pop(0):
            pass_on()

    def consume(p):
        if not waited:
            for load in loads:
                load.wait()
            waited.append(True)
        tokens = slots[p].astype(F32)
        squared = tokens * tokens
        folded = squared[:, :128]
        for k in range(1, features // 128):
            folded = folded + squared[:, k * 128 : (k + 1) * 128]
        squares[...] += folded
        scaled = (tokens * gain_ref[p]).astype(BF16)
        rows = pl.ds(pl.multiple_of(p * features, features), features)
        total[...] += jnp.dot(scaled, held[rows, :], preferred_element_type=F32)

    tp_gather(nx, slots, token_send, token_recv, consume, pause)
    mean = jnp.sum(squares[...], axis=1, keepdims=True) / held.shape[0]
    inverse = lax.rsqrt(mean + EPSILON)

    def projected(number):
        return (total[:, number * 128 : (number + 1) * 128] * inverse).astype(BF16)

    kv = (kbuf, vbuf)

    def a_copy(way, unit, slot, step):
        ref = kv[unit].at[slot]
        target = on_a(shifted(a, 1 if way == 0 else -1))
        return remote(ref, ref, kv_send.at[way, unit, step], kv_recv.at[way, unit, step], target)

    def b_copy(way, slot, step):
        ref = qbuf.at[slot]
        target = on_b(shifted(b, 1 if way == 0 else -1))
        return remote(ref, ref, q_send.at[way, step], q_recv.at[way, step], target)

    def a_units(way, step):
        if 2 * step < size:
            return (0, 1)
        return (0,) if way == 0 else (1,)

    def slot_of(place, way, step):
        return shifted(place, -step if way == 0 else step)

    def b_ways(step):
        return (0, 1) if 2 * step < size else (0,)

    started = []

    def begin(copy):
        copy.start()
        started.append(copy)

    kbuf[a] = projected(4)
    for way in (0, 1):
        begin(a_copy(way, 0, a, 0))
    vbuf[a] = jnp.transpose(projected(5).astype(F32)).astype(BF16)
    for way in (0, 1):
        begin(a_copy(way, 1, a, 0))
    qbuf[b] = jnp.transpose(projected(3).astype(F32) * (FD**-0.5)).astype(BF16)
    for way in (0, 1):
        begin(b_copy(way, b, 0))

    queries = projected(0).astype(F32)
    forget = projected(1).astype(F32)
    values = projected(2)
    inflow = (1.0 - floor_ref[...]) / (1.0 + jnp.exp(forget))
    extra = jnp.transpose(jnp.broadcast_to(decay_ref[...], (128, height)))
    decays = jnp.log1p(-inflow) - extra
    rows_i = lax.broadcasted_iota(jnp.int32, (height, height), 0)
    cols_i = lax.broadcasted_iota(jnp.int32, (height, height), 1)
    lower = jnp.where(cols_i <= rows_i, 1.0, 0.0).astype(BF16)
    sums = jnp.zeros((height, 128), F32)
    for third in thirds(decays):
        sums = sums + jnp.dot(lower, third, preferred_element_type=F32)
    ending = sums[height - 1 : height, :]
    kept = (inflow * jnp.exp(ending - sums)).astype(BF16)
    values_rt = jnp.transpose(values.astype(F32)).astype(BF16)
    own_state = jnp.dot(values_rt, kept, preferred_element_type=F32).astype(BF16)

    part = 128 // size
    logs = padded_thirds([ending], 16)
    for target in range(size):
        slice_out[target] = jnp.concatenate([own_state[target * part : (target + 1) * part], logs], axis=0)
    slice_in[y] = slice_out[y]
    turned = jnp.transpose(start_ref[...])
    for slot in range(size):
        start_t[slot] = turned[slot * part : (slot + 1) * part]

    def slice_copy(source, target):
        return remote(
            slice_out.at[target], slice_in.at[source], s_send.at[target], s_recv.at[source], {"y": target}
        )

    @pl.loop(1, size)
    def _(step):
        slice_copy(y, shifted(y, step)).start()

    mixing = []
    for at in range(0, height, SUB):
        reach = 128 if at + SUB <= 128 else height
        base = sums[at - 1 : at, :] if at else jnp.zeros((1, 128), F32)
        near = queries[at : at + SUB] * jnp.exp(sums[at : at + SUB] - base)
        past = inflow[:reach] * jnp.exp(jnp.minimum(base - sums[:reach], 60.0))
        piece = nt(near.astype(BF16), past.astype(BF16))
        if reach < height:
            piece = jnp.concatenate([piece, jnp.zeros((SUB, height - reach), F32)], axis=1)
        mixing.append(piece)
    mixing = jnp.where(cols_i <= rows_i, jnp.concatenate(mixing, axis=0), 0.0)
    local_out = jnp.dot(mixing.astype(BF16), values, preferred_element_type=F32)
    carried_query = (queries * jnp.exp(sums)).astype(BF16)

    ones = jnp.ones((16, height), BF16)
    blank = jnp.zeros((FD, height), BF16)

    def split_query(iq, head):
        piece = qbuf[iq, head * FD : (head + 1) * FD]
        return jnp.concatenate([piece, blank] if head == 0 else [blank, piece], axis=0)

    def with_ones(ik, head):
        return jnp.concatenate([vbuf[ik, head * FD : (head + 1) * FD], ones], axis=0)

    def wide(column):
        return jnp.concatenate([column] * (height // 128), axis=1)

    def fold_own():
        for head in range(2):
            scores = jnp.dot(kbuf[a], split_query(b, head), preferred_element_type=F32) + wide(bias[a, head])
            scores = jnp.where(rows_i <= cols_i, scores, LOW)
            new = jnp.broadcast_to(jnp.max(scores, axis=0, keepdims=True), (8, height))
            top[b, head] = new
            weights = jnp.exp(scores - new[0:1]).astype(BF16)
            acc[b, head] = jnp.dot(with_ones(a, head), weights, preferred_element_type=F32)

    fold_own()

    def pipeline(count, place):
        def at(number):
            return place(jnp.clip(number, 0, count - 1))

        def scores_of(number, lane):
            iq, ik = at(number)
            keys = kbuf[ik]
            row, column = mine * iq + c * ik, mine * ik + c * iq
            later = jnp.where((row == z) & ((column - y) * (mine - c) > 0), LOW, 0.0)
            for head in range(2):
                scores = jnp.dot(keys, split_query(iq, head), preferred_element_type=F32)
                scores = scores + wide(bias[ik, head] + later)
                old = top[iq, head]
                new = jnp.maximum(old, jnp.max(scores, axis=0, keepdims=True))
                score_s[lane, head] = scores
                top[iq, head] = new
                top_s[lane, head] = new
                scale_s[lane, head] = jnp.exp(old - new)

        def weights_of(lane):
            for head in range(2):
                weight_s[lane, head] = jnp.exp(score_s[lane, head] - top_s[lane, head][0:1]).astype(BF16)
                scale_w[lane, head] = scale_s[lane, head]

        def sums_of(number, lane):
            iq, ik = at(number)
            for head in range(2):
                acc[iq, head] = acc[iq, head] * scale_w[lane, head][0:1] + jnp.dot(
                    with_ones(ik, head), weight_s[lane, head], preferred_element_type=F32
                )

        weight_s[...] = jnp.zeros_like(weight_s)
        scale_w[...] = jnp.ones_like(scale_w)
        for lane in range(LANES):
            scores_of(lane, lane)
        rounds = (count + LANES - 1) // LANES

        def turn(n, carry):
            for lane in range(LANES):
                number = n * LANES + lane
                sums_of(number - LANES, lane)
                weights_of(lane)
                scores_of(number + LANES, lane)
            return carry

        lax.fori_loop(0, rounds, turn, 0)
        for lane in range(LANES):
            number = (rounds - 1) * LANES + lane

            @pl.when(number < count)
            def _(number=number, lane=lane):
                sums_of(number, lane)

    reach = mine * (size - 1 - z) + c * z

    def fold(step):
        last = 2 * step == size
        back = min(step, size // 2 - 1)
        ahead = jnp.minimum(step, reach) + 1
        behind = jnp.maximum(back - (size - 1 - reach), 0)
        fresh = 1 if last else 2
        first = (ahead + behind) * fresh
        one = jnp.where(step <= reach, 1, 0)
        two = 0 if last else jnp.where(size - step <= reach, 1, 0)
        known = 2 * step - 1

        def place(number):
            which = number // fresh
            bounded = jnp.where(which < ahead, which, size - back + which - ahead)
            free = step if last else (number % 2) * (2 * step) - step
            rest = jnp.maximum(number - first, 0)
            bounded_new = jnp.where((rest // known == 0) & (one == 1), step, size - step)
            free_new = rest % known - (step - 1)
            old = number < first
            bounded, free = jnp.where(old, bounded, bounded_new), jnp.where(old, free, free_new)
            iq = mine * (b + bounded) + c * shifted(b, free)
            ik = mine * shifted(a, free) + c * (a - bounded)
            return iq, ik

        pipeline(first + (one + two) * known, place)

    def log_of(block):
        return block[part : part + 1] + block[part + 1 : part + 2] + block[part + 2 : part + 3]

    def total_copy(source, target):
        ref = total_in.at[source]
        return remote(ref, ref, t_send.at[target], t_recv.at[source], {"z": target})

    def state_copy(source, target):
        return remote(state_out.at[target], state_in.at[source], u_send.at[target], u_recv.at[source], {"y": target})

    def row_states():
        @pl.loop(1, size)
        def _(step):
            source = shifted(y, -step)
            slice_copy(source, y).wait_recv()

        state = jnp.zeros((part, 128), F32)
        log_all = jnp.zeros((1, 128), F32)
        for slot in range(size):
            prefix[slot] = state
            log_prefix[slot] = jnp.broadcast_to(log_all, (8, 128))
            block = slice_in[slot].astype(F32)
            log_own = log_of(block)
            state = state * jnp.exp(log_own) + block[:part]
            log_all = log_all + log_own
        total_in[z] = jnp.concatenate([state.astype(BF16), padded_thirds([log_all], 16)], axis=0)

        @pl.loop(z + 1, size)
        def _(target):
            total_copy(z, target).start()

    def all_states():
        def take(slot, state):
            total_copy(slot, z).wait_recv()
            block = total_in[slot].astype(F32)
            return state * jnp.exp(log_of(block)) + block[:part]

        incoming = lax.fori_loop(0, z, take, start_t[y])
        for slot in range(size):
            state = incoming * jnp.exp(log_prefix[slot][0:1]) + prefix[slot]
            state_out[slot] = state.astype(BF16)
        state_in[y] = state_out[y]

        @pl.loop(1, size)
        def _(step):
            state_copy(y, shifted(y, step)).start()

    for step in range(1, size // 2 + 1):
        for unit in (0, 1):
            for way in (0, 1):
                if unit in a_units(way, step):
                    slot = slot_of(a, way, step)
                    a_copy(way, unit, slot, step - 1).wait_recv()
                    if 2 * step < size and unit in a_units(way, step + 1):
                        begin(a_copy(way, unit, slot, step))
        for way in b_ways(step):
            slot = slot_of(b, way, step)
            b_copy(way, slot, step - 1).wait_recv()
            if 2 * step < size and way in b_ways(step + 1):
                begin(b_copy(way, slot, step))
        fold(step)
        if step == 1:
            row_states()
        if step == 2:
            all_states()

    def o_copy(source, slot, target):
        return remote(obuf.at[slot], rbuf.at[source], o_send.at[slot], o_recv.at[source], on_b(target))

    def logs_of(iq):
        shift = query_gates(iq) - reference_gate
        return [
            top[iq, head][0:1] + jnp.log(acc[iq, head][FD : FD + 1]) + shift[head : head + 1] for head in range(2)
        ]

    def rows_of(iq):
        return [acc[iq, head][:FD] / acc[iq, head][FD : FD + 1] for head in range(2)]

    sent = mine * (size - 1 - z) + c * (size - 1)
    received = mine * z + c * (size - 1)

    @pl.loop(1, sent + 1)
    def _(step):
        target = shifted(b, step)
        obuf[target] = jnp.concatenate(
            [piece.astype(BF16) for piece in rows_of(target)] + [padded_thirds(logs_of(target), 16)], axis=0
        )
        o_copy(b, target, target).start()

    @pl.loop(1, size)
    def _(step):
        source = shifted(y, -step)
        state_copy(source, y).wait_recv()

    arriving = jnp.concatenate([state_in[slot] for slot in range(size)], axis=0)
    rec_out = local_out + nt(carried_query, arriving)
    mean = jnp.mean(rec_out * rec_out, axis=1, keepdims=True)
    rows_slots[me, :, 0:128] = (rec_out * lax.rsqrt(mean + EPSILON) * recur_gain_ref[...]).astype(BF16)

    def merge(step, carry):
        slot = shifted(b, -step)
        o_copy(slot, slot, b).wait_recv()
        block = rbuf[slot].astype(F32)
        merged = []
        for head in range(2):
            best, amount, rows = carry[3 * head : 3 * head + 3]
            at = 2 * FD + 3 * head
            log = block[at : at + 1] + block[at + 1 : at + 2] + block[at + 2 : at + 3]
            new = jnp.maximum(best, log)
            keep, add = jnp.exp(best - new), jnp.exp(log - new)
            merged += [new, amount * keep + add, rows * keep + block[head * FD : (head + 1) * FD] * add]
        return tuple(merged)

    own_logs, own_rows = logs_of(b), rows_of(b)
    start = []
    for head in range(2):
        start += [own_logs[head], jnp.ones((1, height), F32), own_rows[head]]
    merged = lax.fori_loop(1, received + 1, merge, tuple(start))
    normed = []
    for head in range(2):
        rows = merged[3 * head + 2] / merged[3 * head + 1]
        mean = jnp.mean(rows * rows, axis=0, keepdims=True)
        normed.append(rows * lax.rsqrt(mean + EPSILON))
    att_rows = jnp.transpose(jnp.concatenate(normed, axis=0))
    rows_slots[me, :, 128:256] = (att_rows * attend_gain_ref[...]).astype(BF16)

    total_out = total.at[:, pl.ds(0, out_ref.shape[1])]
    total_out[...] = jnp.zeros(out_ref.shape, F32)
    for load in output_loads:
        load.wait()

    def consume_rows(p):
        total_out[...] += jnp.dot(rows_slots[p], held_out[p], preferred_element_type=F32)

    tp_gather(nx, rows_slots, rows_send, rows_recv, consume_rows)
    out_ref[...] = total_out[...].astype(BF16)

    for copy in started:
        copy.wait_send()

    @pl.loop(1, size)
    def _(step):
        slice_copy(y, shifted(y, step)).wait_send()
        state_copy(y, shifted(y, step)).wait_send()

    @pl.loop(z + 1, size)
    def _(target):
        total_copy(z, target).wait_send()

    @pl.loop(1, sent + 1)
    def _(step):
        target = shifted(b, step)
        o_copy(b, target, target).wait_send()


VM = pl.BlockSpec(memory_space=pltpu.VMEM)
ANY = pl.BlockSpec(memory_space=pl.ANY)
DMA = pltpu.SemaphoreType.DMA


def params(number):
    return pltpu.CompilerParams(collective_id=number, has_side_effects=True, vmem_limit_bytes=VMEM_LIMIT)


def unpack(size, nx, *refs):
    layer_kernel(size, nx, refs[0], refs[1], refs[2:8], *refs[8:])


def layer(size, nx, tokens, norm_gain, weights, gate_floor, extra_decay, start_state, recur_gain, gate_cache, attend_gain, recur_output, attend_output):
    height, features = tokens.shape
    model = norm_gain.shape[0]
    width = sum(weight.shape[1] for weight in weights)
    out_width = recur_output.shape[1]
    part = 128 // size
    return pl.pallas_call(
        functools.partial(unpack, size, nx),
        out_shape=jax.ShapeDtypeStruct((height, out_width), BF16),
        in_specs=[ANY, VM] + [ANY] * 6 + [VM] * 6 + [ANY] * 2,
        out_specs=VM,
        scratch_shapes=[
            pltpu.VMEM((2 * nx, height, features), BF16),
            pltpu.VMEM((model, width), BF16),
            pltpu.VMEM((height, width), F32),
            pltpu.VMEM((height, 128), F32),
            pltpu.VMEM((2 * nx, height, 256), BF16),
            pltpu.VMEM((2 * nx, 256, out_width), BF16),
            DMA,
            DMA((6,)),
            DMA((4 * nx,)),
            DMA((10,)),
            DMA((10,)),
            DMA((10,)),
            DMA((10,)),
            pltpu.SemaphoreType.REGULAR((4,)),
            pltpu.VMEM((size, height, 128), BF16),
            pltpu.VMEM((size, 128, height), BF16),
            pltpu.VMEM((size, 128, height), BF16),
            pltpu.VMEM((size, part + 16, 128), BF16),
            pltpu.VMEM((size, part + 16, 128), BF16),
            pltpu.VMEM((size, part + 16, 128), BF16),
            pltpu.VMEM((size, part, 128), BF16),
            pltpu.VMEM((size, part, 128), BF16),
            pltpu.VMEM((size, part, 128), F32),
            pltpu.VMEM((size, part, 128), F32),
            pltpu.VMEM((size, 8, 128), F32),
            pltpu.VMEM((size, 144, height), BF16),
            pltpu.VMEM((size, 144, height), BF16),
            pltpu.VMEM((size, 2, FD + 16, height), F32),
            pltpu.VMEM((size, 2, 8, height), F32),
            pltpu.VMEM((size, 2, height, 128), F32),
            pltpu.VMEM((LANES, 2, height, height), F32),
            pltpu.VMEM((LANES, 2, height, height), BF16),
            pltpu.VMEM((LANES, 2, 8, height), F32),
            pltpu.VMEM((LANES, 2, 8, height), F32),
            pltpu.VMEM((LANES, 2, 8, height), F32),
            DMA((2, 2, size // 2)),
            DMA((2, 2, size // 2)),
            DMA((2, size // 2)),
            DMA((2, size // 2)),
        ]
        + [DMA((size,))] * 8,
        compiler_params=params(0),
        name="layer",
    )(
        tokens,
        norm_gain.reshape(2 * nx, 1, features),
        *weights,
        gate_floor.reshape(1, -1),
        extra_decay.reshape(1, -1),
        start_state.reshape(128, 128),
        recur_gain.reshape(1, -1),
        gate_cache.T,
        attend_gain.reshape(1, -1),
        recur_output,
        attend_output,
    )


def shards(
    sizes,
    tokens,
    norm_gain,
    recur_query,
    recur_forget,
    recur_value,
    gate_floor,
    extra_decay,
    start_state,
    recur_gain,
    attend_query,
    attend_key,
    attend_value,
    gate_cache,
    attend_gain,
    recur_output,
    attend_output,
):
    _, ny, nx = sizes
    weights = (recur_query, recur_forget, recur_value, attend_query, attend_key, attend_value)
    return layer(ny, nx, tokens, norm_gain, weights, gate_floor, extra_decay, start_state, recur_gain, gate_cache, attend_gain, recur_output, attend_output)


def solution(mesh):
    sizes = (8, 8, 4)
    finer = Mesh(mesh.devices.reshape(*sizes, 2), ("z", "y", "x", "c"))
    return jax.shard_map(
        functools.partial(shards, sizes),
        mesh=finer,
        in_specs=(
            P(SP, TP),
            P(),
            P(None, TP),
            P(None, TP),
            P(None, TP),
            P(TP),
            P(SP, TP),
            P(TP, None, None),
            P(TP),
            P(None, TP),
            P(None, TP),
            P(None, TP),
            P(None, TP),
            P(TP),
            P(None, TP),
            P(None, TP),
        ),
        out_specs=P(SP, TP),
        check_vma=False,
    )
```

```python
import functools

import jax
import jax.numpy as jnp
from jax import lax
from jax.experimental import pallas as pl
from jax.experimental.pallas import tpu as pltpu
from jax.sharding import Mesh
from jax.sharding import PartitionSpec as P

FD = 64
SP = ("z", "y")
TP = ("x", "c")
EPSILON = 1e-06
LOW = -1e30
SUB = 16
LANES = 2
F32 = jnp.float32
BF16 = jnp.bfloat16
MESH = pl.DeviceIdType.MESH
VMEM_LIMIT = 60 * 1024 * 1024


def remote(src, dst, send, recv, device):
    return pltpu.make_async_remote_copy(
        src_ref=src, dst_ref=dst, send_sem=send, recv_sem=recv, device_id=device, device_id_type=MESH
    )


def tp_gather(nx, slots, send_sem, recv_sem, consume, begun=lambda: None, pause=lambda: None):
    x, c = lax.axis_index("x"), lax.axis_index("c")
    other = 1 - c
    right, left, far = lax.rem(x + 1, nx), lax.rem(x + nx - 1, nx), lax.rem(x + 2, nx)
    half = slots.shape[1] // 2
    me = 2 * x + c
    top, bottom = pl.ds(0, half), pl.ds(half, half)

    def piece(number, p, rows, device):
        ref = slots.at[p] if rows is None else slots.at[p, rows]
        return remote(ref, ref, send_sem.at[number], recv_sem.at[number], device)

    to_right, to_left, to_other = {"x": right}, {"x": left}, {"c": other}
    from_left, from_right, across = 2 * left + c, 2 * right + c, 2 * far + c
    sends = [
        piece(0, me, top, to_right),
        piece(1, me, bottom, to_left),
        piece(2, me, bottom, to_right),
        piece(3, me, top, to_left),
        piece(4, me, None, to_other),
    ]
    for copy in sends:
        copy.start()
    begun()
    consume(me)

    def forward(number, p, rows, device):
        copy = piece(number, p, rows, device)
        copy.start()
        sends.append(copy)

    piece(0, from_left, top, to_right).wait_recv()
    forward(5, from_left, top, to_right)
    piece(1, from_right, bottom, to_left).wait_recv()
    forward(6, from_right, bottom, to_left)
    pause()
    piece(4, 2 * x + other, None, to_other).wait_recv()
    consume(2 * x + other)
    piece(2, from_left, bottom, to_right).wait_recv()
    forward(7, from_left, None, to_other)
    piece(3, from_right, top, to_left).wait_recv()
    forward(8, from_right, None, to_other)
    pause()
    consume(from_left)
    consume(from_right)
    piece(5, across, top, to_right).wait_recv()
    piece(6, across, bottom, to_left).wait_recv()
    forward(9, across, None, to_other)
    pause()
    piece(7, 2 * left + other, None, to_other).wait_recv()
    consume(2 * left + other)
    piece(8, 2 * right + other, None, to_other).wait_recv()
    consume(2 * right + other)
    consume(across)
    piece(9, 2 * far + other, None, to_other).wait_recv()
    consume(2 * far + other)
    for copy in sends:
        copy.wait_send()


def thirds(value):
    first = value.astype(BF16)
    rest = value - first.astype(F32)
    second = rest.astype(BF16)
    third = (rest - second.astype(F32)).astype(BF16)
    return first, second, third


def whole(first, second, third):
    return first.astype(F32) + second.astype(F32) + third.astype(F32)


def padded_thirds(rows, height):
    parts = [part.astype(F32) for row in rows for part in thirds(row)]
    parts.append(jnp.zeros((height - len(parts), rows[0].shape[1]), F32))
    return jnp.concatenate(parts, axis=0).astype(BF16)


def nt(left, right):
    return lax.dot_general(left, right, (((1,), (1,)), ((), ())), preferred_element_type=F32)


def layer_kernel(
    size,
    nx,
    tokens_ref,
    gain_any,
    weight_refs,
    floor_any,
    decay_any,
    start_any,
    recur_gain_any,
    gate_any,
    attend_gain_any,
    recur_output_ref,
    attend_output_ref,
    out_ref,
    slots,
    held,
    total,
    squares,
    rows_slots,
    held_out,
    gain_ref,
    floor_ref,
    decay_ref,
    start_ref,
    recur_gain_ref,
    gate_ref,
    attend_gain_ref,
    small_sem,
    local_sem,
    weight_sem,
    output_sem,
    token_send,
    token_recv,
    rows_send,
    rows_recv,
    chain,
    kbuf,
    vbuf,
    qbuf,
    slice_out,
    slice_in,
    total_in,
    state_out,
    state_in,
    start_t,
    prefix,
    log_prefix,
    obuf,
    rbuf,
    acc,
    top,
    bias,
    score_s,
    weight_s,
    top_s,
    scale_s,
    scale_w,
    kv_send,
    kv_recv,
    q_send,
    q_recv,
    s_send,
    s_recv,
    t_send,
    t_recv,
    u_send,
    u_recv,
    o_send,
    o_recv,
):
    z, y, x, c = (lax.axis_index(name) for name in ("z", "y", "x", "c"))
    height, features = tokens_ref.shape
    me = 2 * x + c

    def shifted(place, offset):
        return lax.rem(place + offset + size, size)

    barrier = pltpu.get_barrier_semaphore()
    along = [{"y": shifted(y, 1)}, {"y": shifted(y, -1)}, {"z": shifted(z, 1)}, {"z": shifted(z, -1)}]
    for device in along + [{"c": 1 - c}, {"x": lax.rem(x + 1, nx)}, {"x": lax.rem(x + nx - 1, nx)}]:
        pl.semaphore_signal(barrier, inc=1, device_id=device, device_id_type=MESH)

    own = pltpu.make_async_copy(tokens_ref, slots.at[me], local_sem)
    own.start()
    width = weight_refs[0].shape[1]
    loads = [
        pltpu.make_async_copy(ref, held.at[:, pl.ds(n * width, width)], weight_sem.at[n])
        for n, ref in enumerate(weight_refs)
    ]
    depth = recur_output_ref.shape[0] // (2 * nx)
    output_loads = [
        pltpu.make_async_copy(
            ref.at[pl.ds(n * depth, depth)], held_out.at[n, pl.ds(k * depth, depth)], output_sem.at[2 * n + k]
        )
        for n in range(2 * nx)
        for k, ref in enumerate((recur_output_ref, attend_output_ref))
    ]
    for load in loads:
        load.start()

    small_loads = [
        pltpu.make_async_copy(source, target, small_sem.at[n])
        for n, (source, target) in enumerate(
            (
                (gain_any, gain_ref),
                (floor_any, floor_ref),
                (decay_any, decay_ref),
                (start_any, start_ref),
                (recur_gain_any, recur_gain_ref),
                (gate_any, gate_ref),
                (attend_gain_any, attend_gain_ref),
            )
        )
    ]
    for load in small_loads + output_loads:
        load.start()

    def pass_on():
        for number, device in enumerate(along):
            pl.semaphore_signal(chain.at[number], inc=1, device_id=device, device_id_type=MESH)

    def hear():
        for number in range(4):
            pl.semaphore_wait(chain.at[number], 1)

    total[...] = jnp.zeros_like(total)
    squares[...] = jnp.zeros_like(squares)

    mine = 1 - c
    a, b = mine * y + c * z, mine * z + c * y

    def on_a(index):
        return {"y": mine * index + c * y, "z": mine * z + c * index}

    def on_b(index):
        return {"z": mine * index + c * z, "y": mine * y + c * index}

    def gates(block):
        return gate_ref[:, pl.ds(pl.multiple_of(block * height, height), height)]

    def key_gates(index):
        return gates(mine * (z * size + index) + c * (index * size + y))

    def query_gates(index):
        return gates(mine * (index * size + y) + c * (z * size + index))

    pl.semaphore_wait(barrier, 7)
    pass_on()
    own.wait()
    waited = []
    rounds_left = [True, True, False]

    def pause():
        hear()
        if rounds_left.pop(0):
            pass_on()

    def consume(p):
        if not waited:
            for load in loads:
                load.wait()
            waited.append(True)
        tokens = slots[p].astype(F32)
        squared = tokens * tokens
        folded = squared[:, :128]
        for k in range(1, features // 128):
            folded = folded + squared[:, k * 128 : (k + 1) * 128]
        squares[...] += folded
        scaled = (tokens * gain_ref[p]).astype(BF16)
        rows = pl.ds(pl.multiple_of(p * features, features), features)
        total[...] += jnp.dot(scaled, held[rows, :], preferred_element_type=F32)

    def prepare():
        for load in small_loads:
            load.wait()
        reference = key_gates(mine * (size - 1) + c * z)[:, height - 1 : height]
        for slot in range(size):
            relative = reference - key_gates(slot)
            for head in range(2):
                bias[slot, head] = jnp.transpose(jnp.broadcast_to(relative[head : head + 1], (128, height)))
        top[...] = jnp.full(top.shape, LOW, F32)
        acc[...] = jnp.zeros_like(acc)

    tp_gather(nx, slots, token_send, token_recv, consume, prepare, pause)
    reference_gate = key_gates(mine * (size - 1) + c * z)[:, height - 1 : height]
    mean = jnp.sum(squares[...], axis=1, keepdims=True) / held.shape[0]
    inverse = lax.rsqrt(mean + EPSILON)

    def projected(number):
        return (total[:, number * 128 : (number + 1) * 128] * inverse).astype(BF16)

    kv = (kbuf, vbuf)

    def a_copy(way, unit, slot, step):
        ref = kv[unit].at[slot]
        target = on_a(shifted(a, 1 if way == 0 else -1))
        return remote(ref, ref, kv_send.at[way, unit, step], kv_recv.at[way, unit, step], target)

    def b_copy(way, slot, step):
        ref = qbuf.at[slot]
        target = on_b(shifted(b, 1 if way == 0 else -1))
        return remote(ref, ref, q_send.at[way, step], q_recv.at[way, step], target)

    def a_units(way, step):
        if 2 * step < size:
            return (0, 1)
        return (0,) if way == 0 else (1,)

    def slot_of(place, way, step):
        return shifted(place, -step if way == 0 else step)

    def b_ways(step):
        return (0, 1) if 2 * step < size else (0,)

    started = []

    def begin(copy):
        copy.start()
        started.append(copy)

    kbuf[a] = projected(4)
    for way in (0, 1):
        begin(a_copy(way, 0, a, 0))
    vbuf[a] = jnp.transpose(projected(5).astype(F32)).astype(BF16)
    for way in (0, 1):
        begin(a_copy(way, 1, a, 0))
    qbuf[b] = jnp.transpose(projected(3).astype(F32) * (FD**-0.5)).astype(BF16)
    for way in (0, 1):
        begin(b_copy(way, b, 0))

    queries = projected(0).astype(F32)
    forget = projected(1).astype(F32)
    values = projected(2)
    inflow = (1.0 - floor_ref[...]) / (1.0 + jnp.exp(forget))
    extra = jnp.transpose(jnp.broadcast_to(decay_ref[...], (128, height)))
    decays = jnp.log1p(-inflow) - extra
    rows_i = lax.broadcasted_iota(jnp.int32, (height, height), 0)
    cols_i = lax.broadcasted_iota(jnp.int32, (height, height), 1)
    lower = jnp.where(cols_i <= rows_i, 1.0, 0.0).astype(BF16)
    sums = jnp.zeros((height, 128), F32)
    for third in thirds(decays):
        sums = sums + jnp.dot(lower, third, preferred_element_type=F32)
    ending = sums[height - 1 : height, :]
    kept = (inflow * jnp.exp(ending - sums)).astype(BF16)
    values_rt = jnp.transpose(values.astype(F32)).astype(BF16)
    own_state = jnp.dot(values_rt, kept, preferred_element_type=F32).astype(BF16)

    part = 128 // size
    logs = padded_thirds([ending], 16)
    for target in range(size):
        slice_out[target] = jnp.concatenate([own_state[target * part : (target + 1) * part], logs], axis=0)
    slice_in[y] = slice_out[y]
    turned = jnp.transpose(start_ref[...])
    for slot in range(size):
        start_t[slot] = turned[slot * part : (slot + 1) * part]

    def slice_copy(source, target):
        return remote(
            slice_out.at[target], slice_in.at[source], s_send.at[target], s_recv.at[source], {"y": target}
        )

    @pl.loop(1, size)
    def _(step):
        slice_copy(y, shifted(y, step)).start()

    mixing = []
    for at in range(0, height, SUB):
        reach = 128 if at + SUB <= 128 else height
        base = sums[at - 1 : at, :] if at else jnp.zeros((1, 128), F32)
        near = queries[at : at + SUB] * jnp.exp(sums[at : at + SUB] - base)
        past = inflow[:reach] * jnp.exp(jnp.minimum(base - sums[:reach], 60.0))
        piece = nt(near.astype(BF16), past.astype(BF16))
        if reach < height:
            piece = jnp.concatenate([piece, jnp.zeros((SUB, height - reach), F32)], axis=1)
        mixing.append(piece)
    mixing = jnp.where(cols_i <= rows_i, jnp.concatenate(mixing, axis=0), 0.0)
    local_out = jnp.dot(mixing.astype(BF16), values, preferred_element_type=F32)
    carried_query = (queries * jnp.exp(sums)).astype(BF16)

    ones = jnp.ones((16, height), BF16)
    blank = jnp.zeros((FD, height), BF16)

    def split_query(iq, head):
        piece = qbuf[iq, head * FD : (head + 1) * FD]
        return jnp.concatenate([piece, blank] if head == 0 else [blank, piece], axis=0)

    def with_ones(ik, head):
        return jnp.concatenate([vbuf[ik, head * FD : (head + 1) * FD], ones], axis=0)

    def wide(column):
        return jnp.concatenate([column] * (height // 128), axis=1)

    def fold_own():
        for head in range(2):
            scores = jnp.dot(kbuf[a], split_query(b, head), preferred_element_type=F32) + wide(bias[a, head])
            scores = jnp.where(rows_i <= cols_i, scores, LOW)
            new = jnp.broadcast_to(jnp.max(scores, axis=0, keepdims=True), (8, height))
            top[b, head] = new
            weights = jnp.exp(scores - new[0:1]).astype(BF16)
            acc[b, head] = jnp.dot(with_ones(a, head), weights, preferred_element_type=F32)

    fold_own()

    def pipeline(count, place):
        def at(number):
            return place(jnp.clip(number, 0, count - 1))

        def scores_of(number, lane):
            iq, ik = at(number)
            keys = kbuf[ik]
            row, column = mine * iq + c * ik, mine * ik + c * iq
            later = jnp.where((row == z) & ((column - y) * (mine - c) > 0), LOW, 0.0)
            for head in range(2):
                scores = jnp.dot(keys, split_query(iq, head), preferred_element_type=F32)
                scores = scores + wide(bias[ik, head] + later)
                old = top[iq, head]
                new = jnp.maximum(old, jnp.max(scores, axis=0, keepdims=True))
                score_s[lane, head] = scores
                top[iq, head] = new
                top_s[lane, head] = new
                scale_s[lane, head] = jnp.exp(old - new)

        def weights_of(lane):
            for head in range(2):
                weight_s[lane, head] = jnp.exp(score_s[lane, head] - top_s[lane, head][0:1]).astype(BF16)
                scale_w[lane, head] = scale_s[lane, head]

        def sums_of(number, lane):
            iq, ik = at(number)
            for head in range(2):
                acc[iq, head] = acc[iq, head] * scale_w[lane, head][0:1] + jnp.dot(
                    with_ones(ik, head), weight_s[lane, head], preferred_element_type=F32
                )

        weight_s[...] = jnp.zeros_like(weight_s)
        scale_w[...] = jnp.ones_like(scale_w)
        for lane in range(LANES):
            scores_of(lane, lane)
        rounds = (count + LANES - 1) // LANES

        def turn(n, carry):
            for lane in range(LANES):
                number = n * LANES + lane
                sums_of(number - LANES, lane)
                weights_of(lane)
                scores_of(number + LANES, lane)
            return carry

        lax.fori_loop(0, rounds, turn, 0)
        for lane in range(LANES):
            number = (rounds - 1) * LANES + lane

            @pl.when(number < count)
            def _(number=number, lane=lane):
                sums_of(number, lane)

    reach = mine * (size - 1 - z) + c * z

    def fold(step):
        last = 2 * step == size
        back = min(step, size // 2 - 1)
        ahead = jnp.minimum(step, reach) + 1
        behind = jnp.maximum(back - (size - 1 - reach), 0)
        fresh = 1 if last else 2
        first = (ahead + behind) * fresh
        one = jnp.where(step <= reach, 1, 0)
        two = 0 if last else jnp.where(size - step <= reach, 1, 0)
        known = 2 * step - 1

        def place(number):
            which = number // fresh
            bounded = jnp.where(which < ahead, which, size - back + which - ahead)
            free = step if last else (number % 2) * (2 * step) - step
            rest = jnp.maximum(number - first, 0)
            bounded_new = jnp.where((rest // known == 0) & (one == 1), step, size - step)
            free_new = rest % known - (step - 1)
            old = number < first
            bounded, free = jnp.where(old, bounded, bounded_new), jnp.where(old, free, free_new)
            iq = mine * (b + bounded) + c * shifted(b, free)
            ik = mine * shifted(a, free) + c * (a - bounded)
            return iq, ik

        pipeline(first + (one + two) * known, place)

    def log_of(block):
        return block[part : part + 1] + block[part + 1 : part + 2] + block[part + 2 : part + 3]

    def total_copy(source, target):
        ref = total_in.at[source]
        return remote(ref, ref, t_send.at[target], t_recv.at[source], {"z": target})

    def state_copy(source, target):
        return remote(state_out.at[target], state_in.at[source], u_send.at[target], u_recv.at[source], {"y": target})

    def row_states():
        @pl.loop(1, size)
        def _(step):
            source = shifted(y, -step)
            slice_copy(source, y).wait_recv()

        state = jnp.zeros((part, 128), F32)
        log_all = jnp.zeros((1, 128), F32)
        for slot in range(size):
            prefix[slot] = state
            log_prefix[slot] = jnp.broadcast_to(log_all, (8, 128))
            block = slice_in[slot].astype(F32)
            log_own = log_of(block)
            state = state * jnp.exp(log_own) + block[:part]
            log_all = log_all + log_own
        total_in[z] = jnp.concatenate([state.astype(BF16), padded_thirds([log_all], 16)], axis=0)

        @pl.loop(z + 1, size)
        def _(target):
            total_copy(z, target).start()

    def all_states():
        def take(slot, state):
            total_copy(slot, z).wait_recv()
            block = total_in[slot].astype(F32)
            return state * jnp.exp(log_of(block)) + block[:part]

        incoming = lax.fori_loop(0, z, take, start_t[y])
        for slot in range(size):
            state = incoming * jnp.exp(log_prefix[slot][0:1]) + prefix[slot]
            state_out[slot] = state.astype(BF16)
        state_in[y] = state_out[y]

        @pl.loop(1, size)
        def _(step):
            state_copy(y, shifted(y, step)).start()

    for step in range(1, size // 2 + 1):
        for unit in (0, 1):
            for way in (0, 1):
                if unit in a_units(way, step):
                    slot = slot_of(a, way, step)
                    a_copy(way, unit, slot, step - 1).wait_recv()
                    if 2 * step < size and unit in a_units(way, step + 1):
                        begin(a_copy(way, unit, slot, step))
        for way in b_ways(step):
            slot = slot_of(b, way, step)
            b_copy(way, slot, step - 1).wait_recv()
            if 2 * step < size and way in b_ways(step + 1):
                begin(b_copy(way, slot, step))
        if step == 2:
            row_states()
        if step == min(3, size // 2):
            all_states()
        if step < size // 2:
            fold(step)

    def o_copy(source, slot, target):
        return remote(obuf.at[slot], rbuf.at[source], o_send.at[slot], o_recv.at[source], on_b(target))

    def logs_of(iq):
        shift = query_gates(iq) - reference_gate
        return [
            top[iq, head][0:1] + jnp.log(acc[iq, head][FD : FD + 1]) + shift[head : head + 1] for head in range(2)
        ]

    def rows_of(iq):
        return [acc[iq, head][:FD] / acc[iq, head][FD : FD + 1] for head in range(2)]

    sent = mine * (size - 1 - z) + c * (size - 1)
    received = mine * z + c * (size - 1)

    half = size // 2
    opposite = jnp.where(half <= reach, 1, 0)

    def give(step):
        target = shifted(b, step)
        obuf[target] = jnp.concatenate(
            [piece.astype(BF16) for piece in rows_of(target)] + [padded_thirds(logs_of(target), 16)], axis=0
        )
        o_copy(b, target, target).start()

    most = mine * (reach + 1 - opposite) + c * opposite * (size - 1)

    def place_most(number):
        bounded = jnp.where(number < half, number, number + 1)
        iq = mine * (b + bounded) + c * shifted(b, number - (half - 1))
        ik = mine * shifted(a, half) + c * (a - half)
        return iq, ik

    @pl.when(most > 0)
    def _():
        pipeline(most, place_most)

    @pl.loop(1, sent + 1)
    def _(step):
        @pl.when(step != half)
        def _():
            give(step)

    rest = mine * opposite * size + c * (reach + 1)

    def place_rest(number):
        return shifted(b, half), mine * shifted(a, number) + c * (a - number)

    @pl.when(rest > 0)
    def _():
        pipeline(rest, place_rest)

    @pl.when(sent >= half)
    def _():
        give(half)

    @pl.loop(1, size)
    def _(step):
        source = shifted(y, -step)
        state_copy(source, y).wait_recv()

    arriving = jnp.concatenate([state_in[slot] for slot in range(size)], axis=0)
    rec_out = local_out + nt(carried_query, arriving)
    mean = jnp.mean(rec_out * rec_out, axis=1, keepdims=True)
    rows_slots[me, :, 0:128] = (rec_out * lax.rsqrt(mean + EPSILON) * recur_gain_ref[...]).astype(BF16)

    def merge(step, carry):
        slot = shifted(b, -step)
        o_copy(slot, slot, b).wait_recv()
        block = rbuf[slot].astype(F32)
        merged = []
        for head in range(2):
            best, amount, rows = carry[3 * head : 3 * head + 3]
            at = 2 * FD + 3 * head
            log = block[at : at + 1] + block[at + 1 : at + 2] + block[at + 2 : at + 3]
            new = jnp.maximum(best, log)
            keep, add = jnp.exp(best - new), jnp.exp(log - new)
            merged += [new, amount * keep + add, rows * keep + block[head * FD : (head + 1) * FD] * add]
        return tuple(merged)

    own_logs, own_rows = logs_of(b), rows_of(b)
    start = []
    for head in range(2):
        start += [own_logs[head], jnp.ones((1, height), F32), own_rows[head]]
    merged = lax.fori_loop(1, received + 1, merge, tuple(start))
    normed = []
    for head in range(2):
        rows = merged[3 * head + 2] / merged[3 * head + 1]
        mean = jnp.mean(rows * rows, axis=0, keepdims=True)
        normed.append(rows * lax.rsqrt(mean + EPSILON))
    att_rows = jnp.transpose(jnp.concatenate(normed, axis=0))
    rows_slots[me, :, 128:256] = (att_rows * attend_gain_ref[...]).astype(BF16)

    total_out = total.at[:, pl.ds(0, out_ref.shape[1])]
    total_out[...] = jnp.zeros(out_ref.shape, F32)
    for load in output_loads:
        load.wait()

    def consume_rows(p):
        total_out[...] += jnp.dot(rows_slots[p], held_out[p], preferred_element_type=F32)

    tp_gather(nx, rows_slots, rows_send, rows_recv, consume_rows)
    out_ref[...] = total_out[...].astype(BF16)

    for copy in started:
        copy.wait_send()

    @pl.loop(1, size)
    def _(step):
        slice_copy(y, shifted(y, step)).wait_send()
        state_copy(y, shifted(y, step)).wait_send()

    @pl.loop(z + 1, size)
    def _(target):
        total_copy(z, target).wait_send()

    @pl.loop(1, sent + 1)
    def _(step):
        target = shifted(b, step)
        o_copy(b, target, target).wait_send()


VM = pl.BlockSpec(memory_space=pltpu.VMEM)
ANY = pl.BlockSpec(memory_space=pl.ANY)
DMA = pltpu.SemaphoreType.DMA


def params(number):
    return pltpu.CompilerParams(collective_id=number, has_side_effects=True, vmem_limit_bytes=VMEM_LIMIT)


def unpack(size, nx, *refs):
    layer_kernel(size, nx, refs[0], refs[1], refs[2:8], *refs[8:])


def layer(size, nx, tokens, norm_gain, weights, gate_floor, extra_decay, start_state, recur_gain, gate_cache, attend_gain, recur_output, attend_output):
    height, features = tokens.shape
    model = norm_gain.shape[0]
    width = sum(weight.shape[1] for weight in weights)
    out_width = recur_output.shape[1]
    part = 128 // size
    return pl.pallas_call(
        functools.partial(unpack, size, nx),
        out_shape=jax.ShapeDtypeStruct((height, out_width), BF16),
        in_specs=[ANY] * 16,
        out_specs=VM,
        scratch_shapes=[
            pltpu.VMEM((2 * nx, height, features), BF16),
            pltpu.VMEM((model, width), BF16),
            pltpu.VMEM((height, width), F32),
            pltpu.VMEM((height, 128), F32),
            pltpu.VMEM((2 * nx, height, 256), BF16),
            pltpu.VMEM((2 * nx, 256, out_width), BF16),
            pltpu.VMEM((2 * nx, 1, features), F32),
            pltpu.VMEM((1, 128), F32),
            pltpu.VMEM((1, height), F32),
            pltpu.VMEM((128, 128), F32),
            pltpu.VMEM((1, 128), F32),
            pltpu.VMEM((2, gate_cache.shape[0]), F32),
            pltpu.VMEM((1, 128), F32),
            DMA((7,)),
            DMA,
            DMA((6,)),
            DMA((4 * nx,)),
            DMA((10,)),
            DMA((10,)),
            DMA((10,)),
            DMA((10,)),
            pltpu.SemaphoreType.REGULAR((4,)),
            pltpu.VMEM((size, height, 128), BF16),
            pltpu.VMEM((size, 128, height), BF16),
            pltpu.VMEM((size, 128, height), BF16),
            pltpu.VMEM((size, part + 16, 128), BF16),
            pltpu.VMEM((size, part + 16, 128), BF16),
            pltpu.VMEM((size, part + 16, 128), BF16),
            pltpu.VMEM((size, part, 128), BF16),
            pltpu.VMEM((size, part, 128), BF16),
            pltpu.VMEM((size, part, 128), F32),
            pltpu.VMEM((size, part, 128), F32),
            pltpu.VMEM((size, 8, 128), F32),
            pltpu.VMEM((size, 144, height), BF16),
            pltpu.VMEM((size, 144, height), BF16),
            pltpu.VMEM((size, 2, FD + 16, height), F32),
            pltpu.VMEM((size, 2, 8, height), F32),
            pltpu.VMEM((size, 2, height, 128), F32),
            pltpu.VMEM((LANES, 2, height, height), F32),
            pltpu.VMEM((LANES, 2, height, height), BF16),
            pltpu.VMEM((LANES, 2, 8, height), F32),
            pltpu.VMEM((LANES, 2, 8, height), F32),
            pltpu.VMEM((LANES, 2, 8, height), F32),
            DMA((2, 2, size // 2)),
            DMA((2, 2, size // 2)),
            DMA((2, size // 2)),
            DMA((2, size // 2)),
        ]
        + [DMA((size,))] * 8,
        compiler_params=params(0),
        name="layer",
    )(
        tokens,
        norm_gain.reshape(2 * nx, 1, features),
        *weights,
        gate_floor.reshape(1, -1),
        extra_decay.reshape(1, -1),
        start_state.reshape(128, 128),
        recur_gain.reshape(1, -1),
        gate_cache.T,
        attend_gain.reshape(1, -1),
        recur_output,
        attend_output,
    )


def shards(
    sizes,
    tokens,
    norm_gain,
    recur_query,
    recur_forget,
    recur_value,
    gate_floor,
    extra_decay,
    start_state,
    recur_gain,
    attend_query,
    attend_key,
    attend_value,
    gate_cache,
    attend_gain,
    recur_output,
    attend_output,
):
    _, ny, nx = sizes
    weights = (recur_query, recur_forget, recur_value, attend_query, attend_key, attend_value)
    return layer(ny, nx, tokens, norm_gain, weights, gate_floor, extra_decay, start_state, recur_gain, gate_cache, attend_gain, recur_output, attend_output)


def solution(mesh):
    sizes = (8, 8, 4)
    finer = Mesh(mesh.devices.reshape(*sizes, 2), ("z", "y", "x", "c"))
    return jax.shard_map(
        functools.partial(shards, sizes),
        mesh=finer,
        in_specs=(
            P(SP, TP),
            P(),
            P(None, TP),
            P(None, TP),
            P(None, TP),
            P(TP),
            P(SP, TP),
            P(TP, None, None),
            P(TP),
            P(None, TP),
            P(None, TP),
            P(None, TP),
            P(None, TP),
            P(TP),
            P(None, TP),
            P(None, TP),
        ),
        out_specs=P(SP, TP),
        check_vma=False,
    )
```

```python
import functools

import jax
import jax.numpy as jnp
from jax import lax
from jax.experimental import pallas as pl
from jax.experimental.pallas import tpu as pltpu
from jax.sharding import Mesh
from jax.sharding import PartitionSpec as P

FD = 64
SP = ("z", "y")
TP = ("x", "c")
EPSILON = 1e-06
LOW = -1e30
SUB = 16
LANES = 2
F32 = jnp.float32
BF16 = jnp.bfloat16
MESH = pl.DeviceIdType.MESH
VMEM_LIMIT = 60 * 1024 * 1024


def remote(src, dst, send, recv, device):
    return pltpu.make_async_remote_copy(
        src_ref=src, dst_ref=dst, send_sem=send, recv_sem=recv, device_id=device, device_id_type=MESH
    )


def tp_gather(nx, slots, send_sem, recv_sem, consume, begun=lambda: None, pause=lambda: None):
    x, c = lax.axis_index("x"), lax.axis_index("c")
    other = 1 - c
    right, left, far = lax.rem(x + 1, nx), lax.rem(x + nx - 1, nx), lax.rem(x + 2, nx)
    half = slots.shape[1] // 2
    me = 2 * x + c
    top, bottom = pl.ds(0, half), pl.ds(half, half)

    def piece(number, p, rows, device):
        ref = slots.at[p] if rows is None else slots.at[p, rows]
        return remote(ref, ref, send_sem.at[number], recv_sem.at[number], device)

    to_right, to_left, to_other = {"x": right}, {"x": left}, {"c": other}
    from_left, from_right, across = 2 * left + c, 2 * right + c, 2 * far + c
    sends = [
        piece(0, me, top, to_right),
        piece(1, me, bottom, to_left),
        piece(2, me, bottom, to_right),
        piece(3, me, top, to_left),
        piece(4, me, None, to_other),
    ]
    for copy in sends:
        copy.start()
    begun()
    consume(me)

    def forward(number, p, rows, device):
        copy = piece(number, p, rows, device)
        copy.start()
        sends.append(copy)

    piece(0, from_left, top, to_right).wait_recv()
    forward(5, from_left, top, to_right)
    piece(1, from_right, bottom, to_left).wait_recv()
    forward(6, from_right, bottom, to_left)
    pause()
    piece(4, 2 * x + other, None, to_other).wait_recv()
    consume(2 * x + other)
    piece(2, from_left, bottom, to_right).wait_recv()
    forward(7, from_left, None, to_other)
    piece(3, from_right, top, to_left).wait_recv()
    forward(8, from_right, None, to_other)
    pause()
    consume(from_left)
    consume(from_right)
    piece(5, across, top, to_right).wait_recv()
    piece(6, across, bottom, to_left).wait_recv()
    forward(9, across, None, to_other)
    pause()
    piece(7, 2 * left + other, None, to_other).wait_recv()
    consume(2 * left + other)
    piece(8, 2 * right + other, None, to_other).wait_recv()
    consume(2 * right + other)
    consume(across)
    piece(9, 2 * far + other, None, to_other).wait_recv()
    consume(2 * far + other)
    for copy in sends:
        copy.wait_send()


def thirds(value):
    first = value.astype(BF16)
    rest = value - first.astype(F32)
    second = rest.astype(BF16)
    third = (rest - second.astype(F32)).astype(BF16)
    return first, second, third


def whole(first, second, third):
    return first.astype(F32) + second.astype(F32) + third.astype(F32)


def padded_thirds(rows, height):
    parts = [part.astype(F32) for row in rows for part in thirds(row)]
    parts.append(jnp.zeros((height - len(parts), rows[0].shape[1]), F32))
    return jnp.concatenate(parts, axis=0).astype(BF16)


def nt(left, right):
    return lax.dot_general(left, right, (((1,), (1,)), ((), ())), preferred_element_type=F32)


def layer_kernel(
    size,
    nx,
    tokens_ref,
    gain_any,
    weight_refs,
    floor_any,
    decay_any,
    start_any,
    recur_gain_any,
    gate_any,
    attend_gain_any,
    recur_output_ref,
    attend_output_ref,
    out_ref,
    slots,
    held,
    total,
    squares,
    rows_slots,
    held_out,
    gain_ref,
    floor_ref,
    decay_ref,
    start_ref,
    recur_gain_ref,
    gate_ref,
    attend_gain_ref,
    small_sem,
    local_sem,
    weight_sem,
    output_sem,
    token_send,
    token_recv,
    rows_send,
    rows_recv,
    chain,
    kbuf,
    vbuf,
    qbuf,
    slice_out,
    slice_in,
    total_in,
    state_out,
    state_in,
    start_t,
    prefix,
    log_prefix,
    obuf,
    rbuf,
    acc,
    top,
    bias,
    score_s,
    weight_s,
    top_s,
    scale_s,
    scale_w,
    kv_send,
    kv_recv,
    q_send,
    q_recv,
    s_send,
    s_recv,
    t_send,
    t_recv,
    u_send,
    u_recv,
    o_send,
    o_recv,
):
    z, y, x, c = (lax.axis_index(name) for name in ("z", "y", "x", "c"))
    height, features = tokens_ref.shape
    me = 2 * x + c

    def shifted(place, offset):
        return lax.rem(place + offset + size, size)

    barrier = pltpu.get_barrier_semaphore()
    along = [{"y": shifted(y, 1)}, {"y": shifted(y, -1)}, {"z": shifted(z, 1)}, {"z": shifted(z, -1)}]
    for device in along + [{"c": 1 - c}, {"x": lax.rem(x + 1, nx)}, {"x": lax.rem(x + nx - 1, nx)}]:
        pl.semaphore_signal(barrier, inc=1, device_id=device, device_id_type=MESH)

    own = pltpu.make_async_copy(tokens_ref, slots.at[me], local_sem)
    own.start()
    width = weight_refs[0].shape[1]
    loads = [
        pltpu.make_async_copy(ref, held.at[:, pl.ds(n * width, width)], weight_sem.at[n])
        for n, ref in enumerate(weight_refs)
    ]
    depth = recur_output_ref.shape[0] // (2 * nx)
    output_loads = [
        pltpu.make_async_copy(
            ref.at[pl.ds(n * depth, depth)], held_out.at[n, pl.ds(k * depth, depth)], output_sem.at[2 * n + k]
        )
        for n in range(2 * nx)
        for k, ref in enumerate((recur_output_ref, attend_output_ref))
    ]
    for load in loads:
        load.start()

    small_loads = [
        pltpu.make_async_copy(source, target, small_sem.at[n])
        for n, (source, target) in enumerate(
            (
                (gain_any, gain_ref),
                (floor_any, floor_ref),
                (decay_any, decay_ref),
                (start_any, start_ref),
                (recur_gain_any, recur_gain_ref),
                (gate_any, gate_ref),
                (attend_gain_any, attend_gain_ref),
            )
        )
    ]
    for load in small_loads + output_loads:
        load.start()

    def pass_on():
        for number, device in enumerate(along):
            pl.semaphore_signal(chain.at[number], inc=1, device_id=device, device_id_type=MESH)

    def hear():
        for number in range(4):
            pl.semaphore_wait(chain.at[number], 1)

    total[...] = jnp.zeros_like(total)
    squares[...] = jnp.zeros_like(squares)

    mine = 1 - c
    a, b = mine * y + c * z, mine * z + c * y

    def on_a(index):
        return {"y": mine * index + c * y, "z": mine * z + c * index}

    def on_b(index):
        return {"z": mine * index + c * z, "y": mine * y + c * index}

    def gates(block):
        return gate_ref[:, pl.ds(pl.multiple_of(block * height, height), height)]

    def key_gates(index):
        return gates(mine * (z * size + index) + c * (index * size + y))

    def query_gates(index):
        return gates(mine * (index * size + y) + c * (z * size + index))

    pl.semaphore_wait(barrier, 7)
    pass_on()
    own.wait()
    waited = []
    rounds_left = [True, True, False]

    def pause():
        hear()
        if rounds_left.pop(0):
            pass_on()

    def consume(p):
        if not waited:
            for load in loads:
                load.wait()
            waited.append(True)
        tokens = slots[p].astype(F32)
        squared = tokens * tokens
        folded = squared[:, :128]
        for k in range(1, features // 128):
            folded = folded + squared[:, k * 128 : (k + 1) * 128]
        squares[...] += folded
        scaled = (tokens * gain_ref[p]).astype(BF16)
        rows = pl.ds(pl.multiple_of(p * features, features), features)
        total[...] += jnp.dot(scaled, held[rows, :], preferred_element_type=F32)

    def prepare():
        for load in small_loads:
            load.wait()
        reference = key_gates(mine * (size - 1) + c * z)[:, height - 1 : height]
        for slot in range(size):
            relative = reference - key_gates(slot)
            for head in range(2):
                bias[slot, head] = jnp.transpose(jnp.broadcast_to(relative[head : head + 1], (128, height)))
        top[...] = jnp.full(top.shape, LOW, F32)
        acc[...] = jnp.zeros_like(acc)

    tp_gather(nx, slots, token_send, token_recv, consume, prepare, pause)
    reference_gate = key_gates(mine * (size - 1) + c * z)[:, height - 1 : height]
    mean = jnp.sum(squares[...], axis=1, keepdims=True) / held.shape[0]
    inverse = lax.rsqrt(mean + EPSILON)

    def projected(number):
        return (total[:, number * 128 : (number + 1) * 128] * inverse).astype(BF16)

    kv = (kbuf, vbuf)

    def a_copy(way, unit, slot, step):
        ref = kv[unit].at[slot]
        target = on_a(shifted(a, 1 if way == 0 else -1))
        return remote(ref, ref, kv_send.at[way, unit, step], kv_recv.at[way, unit, step], target)

    def b_copy(way, slot, step):
        ref = qbuf.at[slot]
        target = on_b(shifted(b, 1 if way == 0 else -1))
        return remote(ref, ref, q_send.at[way, step], q_recv.at[way, step], target)

    def a_units(way, step):
        if 2 * step < size:
            return (0, 1)
        return (0,) if way == 0 else (1,)

    def slot_of(place, way, step):
        return shifted(place, -step if way == 0 else step)

    def b_ways(step):
        return (0, 1) if 2 * step < size else (0,)

    started = []

    def begin(copy):
        copy.start()
        started.append(copy)

    kbuf[a] = projected(4)
    for way in (0, 1):
        begin(a_copy(way, 0, a, 0))
    vbuf[a] = jnp.transpose(projected(5).astype(F32)).astype(BF16)
    for way in (0, 1):
        begin(a_copy(way, 1, a, 0))
    qbuf[b] = jnp.transpose(projected(3).astype(F32) * (FD**-0.5)).astype(BF16)
    for way in (0, 1):
        begin(b_copy(way, b, 0))

    queries = projected(0).astype(F32)
    forget = projected(1).astype(F32)
    values = projected(2)
    inflow = (1.0 - floor_ref[...]) / (1.0 + jnp.exp(forget))
    extra = jnp.transpose(jnp.broadcast_to(decay_ref[...], (128, height)))
    decays = jnp.log1p(-inflow) - extra
    rows_i = lax.broadcasted_iota(jnp.int32, (height, height), 0)
    cols_i = lax.broadcasted_iota(jnp.int32, (height, height), 1)
    lower = jnp.where(cols_i <= rows_i, 1.0, 0.0).astype(BF16)
    sums = jnp.zeros((height, 128), F32)
    for third in thirds(decays):
        sums = sums + jnp.dot(lower, third, preferred_element_type=F32)
    ending = sums[height - 1 : height, :]
    kept = (inflow * jnp.exp(ending - sums)).astype(BF16)
    values_rt = jnp.transpose(values.astype(F32)).astype(BF16)
    own_state = jnp.dot(values_rt, kept, preferred_element_type=F32).astype(BF16)

    part = 128 // size
    logs = padded_thirds([ending], 16)
    for target in range(size):
        slice_out[target] = jnp.concatenate([own_state[target * part : (target + 1) * part], logs], axis=0)
    slice_in[y] = slice_out[y]
    turned = jnp.transpose(start_ref[...])
    for slot in range(size):
        start_t[slot] = turned[slot * part : (slot + 1) * part]

    def slice_copy(source, target):
        return remote(
            slice_out.at[target], slice_in.at[source], s_send.at[target], s_recv.at[source], {"y": target}
        )

    @pl.loop(1, size)
    def _(step):
        slice_copy(y, shifted(y, step)).start()

    mixing = []
    for at in range(0, height, SUB):
        reach = 128 if at + SUB <= 128 else height
        base = sums[at - 1 : at, :] if at else jnp.zeros((1, 128), F32)
        near = queries[at : at + SUB] * jnp.exp(sums[at : at + SUB] - base)
        past = inflow[:reach] * jnp.exp(jnp.minimum(base - sums[:reach], 60.0))
        piece = nt(near.astype(BF16), past.astype(BF16))
        if reach < height:
            piece = jnp.concatenate([piece, jnp.zeros((SUB, height - reach), F32)], axis=1)
        mixing.append(piece)
    mixing = jnp.where(cols_i <= rows_i, jnp.concatenate(mixing, axis=0), 0.0)
    local_out = jnp.dot(mixing.astype(BF16), values, preferred_element_type=F32)
    carried_query = (queries * jnp.exp(sums)).astype(BF16)

    ones = jnp.ones((16, height), BF16)
    blank = jnp.zeros((FD, height), BF16)

    def split_query(iq, head):
        piece = qbuf[iq, head * FD : (head + 1) * FD]
        return jnp.concatenate([piece, blank] if head == 0 else [blank, piece], axis=0)

    def with_ones(ik, head):
        return jnp.concatenate([vbuf[ik, head * FD : (head + 1) * FD], ones], axis=0)

    def wide(column):
        return jnp.concatenate([column] * (height // 128), axis=1)

    def fold_own():
        for head in range(2):
            scores = jnp.dot(kbuf[a], split_query(b, head), preferred_element_type=F32) + wide(bias[a, head])
            scores = jnp.where(rows_i <= cols_i, scores, LOW)
            new = jnp.broadcast_to(jnp.max(scores, axis=0, keepdims=True), (8, height))
            top[b, head] = new
            weights = jnp.exp(scores - new[0:1]).astype(BF16)
            acc[b, head] = jnp.dot(with_ones(a, head), weights, preferred_element_type=F32)

    fold_own()

    def pipeline(count, place):
        def at(number):
            return place(jnp.clip(number, 0, count - 1))

        def scores_of(number, lane):
            iq, ik = at(number)
            keys = kbuf[ik]
            row, column = mine * iq + c * ik, mine * ik + c * iq
            later = jnp.where((row == z) & ((column - y) * (mine - c) > 0), LOW, 0.0)
            for head in range(2):
                scores = jnp.dot(keys, split_query(iq, head), preferred_element_type=F32)
                scores = scores + wide(bias[ik, head] + later)
                old = top[iq, head]
                new = jnp.maximum(old, jnp.max(scores, axis=0, keepdims=True))
                score_s[lane, head] = scores
                top[iq, head] = new
                top_s[lane, head] = new
                scale_s[lane, head] = jnp.exp(old - new)

        def weights_of(lane):
            for head in range(2):
                weight_s[lane, head] = jnp.exp(score_s[lane, head] - top_s[lane, head][0:1]).astype(BF16)
                scale_w[lane, head] = scale_s[lane, head]

        def sums_of(number, lane):
            iq, ik = at(number)
            for head in range(2):
                acc[iq, head] = acc[iq, head] * scale_w[lane, head][0:1] + jnp.dot(
                    with_ones(ik, head), weight_s[lane, head], preferred_element_type=F32
                )

        weight_s[...] = jnp.zeros_like(weight_s)
        scale_w[...] = jnp.ones_like(scale_w)
        for lane in range(LANES):
            scores_of(lane, lane)
        rounds = (count + LANES - 1) // LANES

        def turn(n, carry):
            for lane in range(LANES):
                number = n * LANES + lane
                sums_of(number - LANES, lane)
                weights_of(lane)
                scores_of(number + LANES, lane)
            return carry

        lax.fori_loop(0, rounds, turn, 0)
        for lane in range(LANES):
            number = (rounds - 1) * LANES + lane

            @pl.when(number < count)
            def _(number=number, lane=lane):
                sums_of(number, lane)

    reach = mine * (size - 1 - z) + c * z

    def fold(step):
        last = 2 * step == size
        back = min(step, size // 2 - 1)
        ahead = jnp.minimum(step, reach) + 1
        behind = jnp.maximum(back - (size - 1 - reach), 0)
        fresh = 1 if last else 2
        first = (ahead + behind) * fresh
        one = jnp.where(step <= reach, 1, 0)
        two = 0 if last else jnp.where(size - step <= reach, 1, 0)
        known = 2 * step - 1

        def place(number):
            which = number // fresh
            bounded = jnp.where(which < ahead, which, size - back + which - ahead)
            free = step if last else (number % 2) * (2 * step) - step
            rest = jnp.maximum(number - first, 0)
            bounded_new = jnp.where((rest // known == 0) & (one == 1), step, size - step)
            free_new = rest % known - (step - 1)
            old = number < first
            bounded, free = jnp.where(old, bounded, bounded_new), jnp.where(old, free, free_new)
            iq = mine * (b + bounded) + c * shifted(b, free)
            ik = mine * shifted(a, free) + c * (a - bounded)
            return iq, ik

        pipeline(first + (one + two) * known, place)

    def log_of(block):
        return block[part : part + 1] + block[part + 1 : part + 2] + block[part + 2 : part + 3]

    def total_copy(source, target):
        ref = total_in.at[source]
        return remote(ref, ref, t_send.at[target], t_recv.at[source], {"z": target})

    def state_copy(source, target):
        return remote(state_out.at[target], state_in.at[source], u_send.at[target], u_recv.at[source], {"y": target})

    def row_states():
        @pl.loop(1, size)
        def _(step):
            source = shifted(y, -step)
            slice_copy(source, y).wait_recv()

        state = jnp.zeros((part, 128), F32)
        log_all = jnp.zeros((1, 128), F32)
        for slot in range(size):
            prefix[slot] = state
            log_prefix[slot] = jnp.broadcast_to(log_all, (8, 128))
            block = slice_in[slot].astype(F32)
            log_own = log_of(block)
            state = state * jnp.exp(log_own) + block[:part]
            log_all = log_all + log_own
        total_in[z] = jnp.concatenate([state.astype(BF16), padded_thirds([log_all], 16)], axis=0)

        @pl.loop(z + 1, size)
        def _(target):
            total_copy(z, target).start()

    def all_states():
        def take(slot, state):
            total_copy(slot, z).wait_recv()
            block = total_in[slot].astype(F32)
            return state * jnp.exp(log_of(block)) + block[:part]

        incoming = lax.fori_loop(0, z, take, start_t[y])
        for slot in range(size):
            state = incoming * jnp.exp(log_prefix[slot][0:1]) + prefix[slot]
            state_out[slot] = state.astype(BF16)
        state_in[y] = state_out[y]

        @pl.loop(1, size)
        def _(step):
            state_copy(y, shifted(y, step)).start()

    for step in range(1, size // 2 + 1):
        for unit in (0, 1):
            for way in (0, 1):
                if unit in a_units(way, step):
                    slot = slot_of(a, way, step)
                    a_copy(way, unit, slot, step - 1).wait_recv()
                    if 2 * step < size and unit in a_units(way, step + 1):
                        begin(a_copy(way, unit, slot, step))
        for way in b_ways(step):
            slot = slot_of(b, way, step)
            b_copy(way, slot, step - 1).wait_recv()
            if 2 * step < size and way in b_ways(step + 1):
                begin(b_copy(way, slot, step))
        if step == 2:
            row_states()
        if step == min(3, size // 2):
            all_states()
        if step < size // 2:
            fold(step)

    def o_copy(source, slot, target):
        return remote(obuf.at[slot], rbuf.at[source], o_send.at[slot], o_recv.at[source], on_b(target))

    def logs_of(iq):
        shift = query_gates(iq) - reference_gate
        return [
            top[iq, head][0:1] + jnp.log(acc[iq, head][FD : FD + 1]) + shift[head : head + 1] for head in range(2)
        ]

    def rows_of(iq):
        return [acc[iq, head][:FD] * (1.0 / acc[iq, head][FD : FD + 1]) for head in range(2)]

    sent = mine * (size - 1 - z) + c * (size - 1)
    received = mine * z + c * (size - 1)

    half = size // 2
    opposite = jnp.where(half <= reach, 1, 0)

    def give(step):
        target = shifted(b, step)
        obuf[target] = jnp.concatenate(
            [piece.astype(BF16) for piece in rows_of(target)] + [padded_thirds(logs_of(target), 16)], axis=0
        )
        o_copy(b, target, target).start()

    most = mine * (reach + 1 - opposite) + c * opposite * (size - 1)

    def place_most(number):
        bounded = jnp.where(number < half, number, number + 1)
        iq = mine * (b + bounded) + c * shifted(b, number - (half - 1))
        ik = mine * shifted(a, half) + c * (a - half)
        return iq, ik

    @pl.when(most > 0)
    def _():
        pipeline(most, place_most)

    @pl.loop(1, sent + 1)
    def _(step):
        @pl.when(step != half)
        def _():
            give(step)

    rest = mine * opposite * size + c * (reach + 1)

    def place_rest(number):
        return shifted(b, half), mine * shifted(a, number) + c * (a - number)

    @pl.when(rest > 0)
    def _():
        pipeline(rest, place_rest)

    @pl.when(sent >= half)
    def _():
        give(half)

    @pl.loop(1, size)
    def _(step):
        source = shifted(y, -step)
        state_copy(source, y).wait_recv()

    arriving = jnp.concatenate([state_in[slot] for slot in range(size)], axis=0)
    rec_out = local_out + nt(carried_query, arriving)
    mean = jnp.mean(rec_out * rec_out, axis=1, keepdims=True)
    rows_slots[me, :, 0:128] = (rec_out * lax.rsqrt(mean + EPSILON) * recur_gain_ref[...]).astype(BF16)

    def merge(step, carry):
        slot = shifted(b, -step)
        o_copy(slot, slot, b).wait_recv()
        block = rbuf[slot].astype(F32)
        merged = []
        for head in range(2):
            best, amount, rows = carry[3 * head : 3 * head + 3]
            at = 2 * FD + 3 * head
            log = block[at : at + 1] + block[at + 1 : at + 2] + block[at + 2 : at + 3]
            new = jnp.maximum(best, log)
            keep, add = jnp.exp(best - new), jnp.exp(log - new)
            merged += [new, amount * keep + add, rows * keep + block[head * FD : (head + 1) * FD] * add]
        return tuple(merged)

    own_logs, own_rows = logs_of(b), rows_of(b)
    start = []
    for head in range(2):
        start += [own_logs[head], jnp.ones((1, height), F32), own_rows[head]]
    merged = lax.fori_loop(1, received + 1, merge, tuple(start))
    normed = []
    for head in range(2):
        rows = merged[3 * head + 2] * (1.0 / merged[3 * head + 1])
        mean = jnp.mean(rows * rows, axis=0, keepdims=True)
        normed.append(rows * lax.rsqrt(mean + EPSILON))
    att_rows = jnp.transpose(jnp.concatenate(normed, axis=0))
    rows_slots[me, :, 128:256] = (att_rows * attend_gain_ref[...]).astype(BF16)

    total_out = total.at[:, pl.ds(0, out_ref.shape[1])]
    total_out[...] = jnp.zeros(out_ref.shape, F32)
    for load in output_loads:
        load.wait()

    def consume_rows(p):
        total_out[...] += jnp.dot(rows_slots[p], held_out[p], preferred_element_type=F32)

    tp_gather(nx, rows_slots, rows_send, rows_recv, consume_rows)
    out_ref[...] = total_out[...].astype(BF16)

    for copy in started:
        copy.wait_send()

    @pl.loop(1, size)
    def _(step):
        slice_copy(y, shifted(y, step)).wait_send()
        state_copy(y, shifted(y, step)).wait_send()

    @pl.loop(z + 1, size)
    def _(target):
        total_copy(z, target).wait_send()

    @pl.loop(1, sent + 1)
    def _(step):
        target = shifted(b, step)
        o_copy(b, target, target).wait_send()


VM = pl.BlockSpec(memory_space=pltpu.VMEM)
ANY = pl.BlockSpec(memory_space=pl.ANY)
DMA = pltpu.SemaphoreType.DMA


def params(number):
    return pltpu.CompilerParams(collective_id=number, has_side_effects=True, vmem_limit_bytes=VMEM_LIMIT)


def unpack(size, nx, *refs):
    layer_kernel(size, nx, refs[0], refs[1], refs[2:8], *refs[8:])


def layer(size, nx, tokens, norm_gain, weights, gate_floor, extra_decay, start_state, recur_gain, gate_cache, attend_gain, recur_output, attend_output):
    height, features = tokens.shape
    model = norm_gain.shape[0]
    width = sum(weight.shape[1] for weight in weights)
    out_width = recur_output.shape[1]
    part = 128 // size
    return pl.pallas_call(
        functools.partial(unpack, size, nx),
        out_shape=jax.ShapeDtypeStruct((height, out_width), BF16),
        in_specs=[ANY] * 16,
        out_specs=VM,
        scratch_shapes=[
            pltpu.VMEM((2 * nx, height, features), BF16),
            pltpu.VMEM((model, width), BF16),
            pltpu.VMEM((height, width), F32),
            pltpu.VMEM((height, 128), F32),
            pltpu.VMEM((2 * nx, height, 256), BF16),
            pltpu.VMEM((2 * nx, 256, out_width), BF16),
            pltpu.VMEM((2 * nx, 1, features), F32),
            pltpu.VMEM((1, 128), F32),
            pltpu.VMEM((1, height), F32),
            pltpu.VMEM((128, 128), F32),
            pltpu.VMEM((1, 128), F32),
            pltpu.VMEM((2, gate_cache.shape[0]), F32),
            pltpu.VMEM((1, 128), F32),
            DMA((7,)),
            DMA,
            DMA((6,)),
            DMA((4 * nx,)),
            DMA((10,)),
            DMA((10,)),
            DMA((10,)),
            DMA((10,)),
            pltpu.SemaphoreType.REGULAR((4,)),
            pltpu.VMEM((size, height, 128), BF16),
            pltpu.VMEM((size, 128, height), BF16),
            pltpu.VMEM((size, 128, height), BF16),
            pltpu.VMEM((size, part + 16, 128), BF16),
            pltpu.VMEM((size, part + 16, 128), BF16),
            pltpu.VMEM((size, part + 16, 128), BF16),
            pltpu.VMEM((size, part, 128), BF16),
            pltpu.VMEM((size, part, 128), BF16),
            pltpu.VMEM((size, part, 128), F32),
            pltpu.VMEM((size, part, 128), F32),
            pltpu.VMEM((size, 8, 128), F32),
            pltpu.VMEM((size, 144, height), BF16),
            pltpu.VMEM((size, 144, height), BF16),
            pltpu.VMEM((size, 2, FD + 16, height), F32),
            pltpu.VMEM((size, 2, 8, height), F32),
            pltpu.VMEM((size, 2, height, 128), F32),
            pltpu.VMEM((LANES, 2, height, height), F32),
            pltpu.VMEM((LANES, 2, height, height), BF16),
            pltpu.VMEM((LANES, 2, 8, height), F32),
            pltpu.VMEM((LANES, 2, 8, height), F32),
            pltpu.VMEM((LANES, 2, 8, height), F32),
            DMA((2, 2, size // 2)),
            DMA((2, 2, size // 2)),
            DMA((2, size // 2)),
            DMA((2, size // 2)),
        ]
        + [DMA((size,))] * 8,
        compiler_params=params(0),
        name="layer",
    )(
        tokens,
        norm_gain.reshape(2 * nx, 1, features),
        *weights,
        gate_floor.reshape(1, -1),
        extra_decay.reshape(1, -1),
        start_state.reshape(128, 128),
        recur_gain.reshape(1, -1),
        gate_cache.T,
        attend_gain.reshape(1, -1),
        recur_output,
        attend_output,
    )


def shards(
    sizes,
    tokens,
    norm_gain,
    recur_query,
    recur_forget,
    recur_value,
    gate_floor,
    extra_decay,
    start_state,
    recur_gain,
    attend_query,
    attend_key,
    attend_value,
    gate_cache,
    attend_gain,
    recur_output,
    attend_output,
):
    _, ny, nx = sizes
    weights = (recur_query, recur_forget, recur_value, attend_query, attend_key, attend_value)
    return layer(ny, nx, tokens, norm_gain, weights, gate_floor, extra_decay, start_state, recur_gain, gate_cache, attend_gain, recur_output, attend_output)


def solution(mesh):
    sizes = (8, 8, 4)
    finer = Mesh(mesh.devices.reshape(*sizes, 2), ("z", "y", "x", "c"))
    return jax.shard_map(
        functools.partial(shards, sizes),
        mesh=finer,
        in_specs=(
            P(SP, TP),
            P(),
            P(None, TP),
            P(None, TP),
            P(None, TP),
            P(TP),
            P(SP, TP),
            P(TP, None, None),
            P(TP),
            P(None, TP),
            P(None, TP),
            P(None, TP),
            P(None, TP),
            P(TP),
            P(None, TP),
            P(None, TP),
        ),
        out_specs=P(SP, TP),
        check_vma=False,
    )
```
